256 devices in a mesh: ep: 128 (over z, y, x), tp: 2 (over core).
Axes of the slice: x: 4, y: 4, z: 8, core: 2. Of those that a mesh axis runs over, the one named last changes fastest.
Arguments:
- tokens: bfloat16 [2048, 2048], P('ep', 'tp'), may hold values from -6 to 6
- state: float32 [2048, 4, 128, 128], P('ep', 'tp'), may hold values from -4 to 4
- norm_mix: float32 [2048], replicated, may hold values from 0.1 to 1.9
- w_query: bfloat16 [2048, 512], P(None, 'tp'), may hold values from -0.125 to 0.125
- w_key: bfloat16 [2048, 512], P(None, 'tp'), may hold values from -0.125 to 0.125
- w_value: bfloat16 [2048, 512], P(None, 'tp'), may hold values from -0.125 to 0.125
- w_out: bfloat16 [512, 2048], P('tp'), may hold values from -0.25 to 0.25
- norm_ffn: float32 [2048], P('tp'), may hold values from 0.1 to 1.9
- gate_vector: bfloat16 [2048], P('tp'), may hold values from -0.125 to 0.125
- dense_gate: bfloat16 [2048, 2816], P('tp', 'ep'), may hold values from -0.125 to 0.125
- dense_up: bfloat16 [2048, 2816], P('tp', 'ep'), may hold values from -0.125 to 0.125
- dense_down: bfloat16 [2816, 2048], P('ep', 'tp'), may hold values from -0.109375 to 0.109375
- exp_gate: bfloat16 [128, 2048, 176], P('ep', None, 'tp'), may hold values from -0.125 to 0.125
- exp_up: bfloat16 [128, 2048, 176], P('ep', None, 'tp'), may hold values from -0.125 to 0.125
- exp_down: bfloat16 [128, 176, 2048], P('ep', 'tp'), may hold values from -0.109375 to 0.109375
- routes: int32 [2048, 2], P('ep'), may hold values from 0 to 7, all different within a row; in each aligned block of 16 rows (0 to 15, 16 to 31, ...) at most 5 rows name the same one
- route_w: bfloat16 [2048, 2], P('ep'), may hold values from 0.099609375 to 1
Outputs:
- mixed: bfloat16 [2048, 2048], P('ep', 'tp')
- new_state: float32 [2048, 4, 128, 128], P('ep', 'tp')
The draws below stay inside these ranges and needn't reach their ends.
Inputs may be any that keep to these rules, and one draw needn't show every extreme that they name: `routes`: each row names 2 different experts. Within the rows of one device (aligned blocks of 16 rows) no expert is named by more than 5 rows, a bound that some blocks reach.
All inputs are finite; a program needn't handle non-finite values.
Results may differ from the reference program's by a relative error of at most 0.014.
Values may be sent and summed in bfloat16 or wider, within the bound.
No kernel may reach another device: no remote copies, remote signals or barrier semaphores. Data moves between devices by JAX's collectives and lax.ppermute only.
A program may use at most 128 MiB of HBM per device.

```python
import math
import jax
import jax.numpy as jnp
import numpy as np
from jax import lax

D = 2048
HEADS = 4
HEAD = 128
FF = 2816
FF_D = 2816
EXPERTS = 8
TOPK = 2
SEQ_DEV = 16
CAP = 5
E_SPLIT = 16
TOKENS = 2048
N_EP = 128
N_TP = 2


def levels(own_key, shape, pieces, low, largest):
    level = 1.0
    for dim, blocks in pieces:
        draws = jax.random.uniform(jax.random.fold_in(jax.random.fold_in(own_key, 6), dim), (blocks,), jnp.float32, low / len(pieces), largest / len(pieces))
        level = level * jnp.repeat(jnp.exp(draws), shape[dim] // blocks).reshape((-1,) + (1,) * (len(shape) - 1 - dim))
    return level


def shared_out(own_key, own, number, rows, count, top, reach, lean):
    order = jax.random.permutation(own_key, count)
    packed, usual = shares(count, rows * top, reach, lean, True), shares(count, rows * top, reach, lean, False)
    places = jnp.arange(count)

    def named(lengths, turn):
        used = int((lengths > 0).sum())
        fixed = max(1, used // 4)
        moved = fixed + (places - fixed + turn * (used - fixed)) % max(1, count - fixed)
        return jnp.zeros((count,), jnp.int32).at[order[jnp.where(places < fixed, places, moved)]].set(jnp.asarray(lengths, jnp.int32))

    lengths = jnp.where(number % 4 == 0, named(packed, number // 4), named(usual, number - number // 4 - 1))
    mixed = jax.random.permutation(jax.random.fold_in(own, 3), count)
    donor, taker = mixed[0:count // 2 * 2:2], mixed[1:count // 2 * 2:2]
    slack = jnp.minimum(lengths[donor] - 1, reach - lengths[taker]) // 2
    slack = jnp.where((donor == order[0]) | (taker == order[0]) | (lengths[taker] == 0), 0, jnp.maximum(slack, 0))
    moved = jax.random.randint(jax.random.fold_in(own, 4), (count // 2,), 0, 1 << 20) % (slack + 1)
    lengths = lengths.at[donor].add(-moved).at[taker].add(moved)
    labels = jnp.searchsorted(jnp.cumsum(lengths), jnp.arange(rows * top), side="right").astype(jnp.int32)
    listing = labels.reshape(top, rows).T
    listing = listing[jax.random.permutation(jax.random.fold_in(own, 1), rows)]
    turn = jax.random.randint(jax.random.fold_in(own, 2), (rows, 1), 0, top)
    return jnp.take_along_axis(listing, (jnp.arange(top)[None, :] + turn) % top, axis=1)


def shares(number_of, total, bound, slope, full):
    loads = [(1 << 20) // math.isqrt(grade ** slope) + 1 for grade in range(1, number_of + 1)]
    largest = bound if full else min(bound, max(-(-total // number_of), total * loads[0] // sum(loads)))
    least = 1 if total - largest >= number_of - 1 else 0
    counts, spare = [largest] + [least] * (number_of - 1), total - largest - least * (number_of - 1)
    while spare > 0:
        free = [i for i in range(1, number_of) if counts[i] < largest] or [i for i in range(1, number_of) if counts[i] < bound]
        whole, left = sum([loads[i] for i in free]), spare
        for i in free:
            extra = min(bound - counts[i], max(1, left * loads[i] // whole), spare)
            counts[i] = counts[i] + extra
            spare = spare - extra
    return np.array(counts)


def gaussian(own_key, dims, scale, bound, cuts=(), kind=jnp.bfloat16):
    level = levels(own_key, dims, cuts, -0.22, 0.18) if cuts else 1.0
    entries = jax.random.normal(own_key, dims, jnp.float32) * scale * level
    return jnp.minimum(jnp.maximum(entries, -bound), bound).astype(kind)


def setup_inputs(seed: int = 0) -> dict:
    seeds = jax.random.split(jax.random.key(seed), 18)
    tokens = gaussian(seeds[0], (TOKENS, D), 1.0, 6.0, ((0, 128), (1, 2)))
    state = gaussian(seeds[1], (TOKENS, HEADS, HEAD, HEAD), 0.5, 4.0, ((0, 128), (1, 2)), jnp.float32)
    norm_mix = jnp.clip(1.0 + 0.18 * jax.random.normal(seeds[2], (D,), jnp.float32), 0.1, 1.9)
    w_query = gaussian(seeds[3], (D, HEADS * HEAD), D ** -0.5, 0.125, ((1, 2),))
    w_key = gaussian(seeds[4], (D, HEADS * HEAD), D ** -0.5, 0.125, ((1, 2),))
    w_value = gaussian(seeds[5], (D, HEADS * HEAD), D ** -0.5, 0.125, ((1, 2),))
    w_out = gaussian(seeds[6], (HEADS * HEAD, D), (HEADS * HEAD) ** -0.5, 0.25, ((0, 2),))
    norm_ffn = jnp.clip(1.0 + 0.18 * jax.random.normal(seeds[7], (D,), jnp.float32), 0.1, 1.9)
    gate_vector = gaussian(seeds[8], (D,), D ** -0.5, 0.125, ((0, 2),))
    dense_gate = gaussian(seeds[9], (D, FF_D), D ** -0.5, 0.125, ((0, 2), (1, 128)))
    dense_up = gaussian(seeds[10], (D, FF_D), D ** -0.5, 0.125, ((0, 2), (1, 128)))
    dense_down = gaussian(seeds[11], (FF_D, D), FF_D ** -0.5, 0.109375, ((0, 128), (1, 2)))
    exp_gate = gaussian(seeds[12], (EXPERTS * E_SPLIT, D, FF // E_SPLIT), D ** -0.5, 0.125, ((0, 128), (2, 2)))
    exp_up = gaussian(seeds[13], (EXPERTS * E_SPLIT, D, FF // E_SPLIT), D ** -0.5, 0.125, ((0, 128), (2, 2)))
    exp_down = gaussian(seeds[14], (EXPERTS * E_SPLIT, FF // E_SPLIT, D), FF ** -0.5, 0.109375, ((0, 128), (1, 2)))
    routes_keys = jax.random.split(jax.random.fold_in(seeds[15], 1), TOKENS // SEQ_DEV)
    routes_turns = jax.random.permutation(jax.random.fold_in(seeds[15], 3), TOKENS // SEQ_DEV)
    routes = jax.vmap(lambda own, number: shared_out(jax.random.fold_in(seeds[15], 2), own, number, SEQ_DEV, EXPERTS, TOPK, CAP, 1))(routes_keys, routes_turns).reshape((TOKENS, TOPK))
    route_w = jnp.clip(0.099609375 + 0.9003906 * jax.random.uniform(seeds[16], (TOKENS, TOPK), jnp.float32) ** levels(seeds[16], (TOKENS, TOPK), ((0, 128),), -0.2, 0.2), 0.099609375, 1.0).astype(jnp.bfloat16)
    return dict(tokens=tokens, state=state, norm_mix=norm_mix, w_query=w_query, w_key=w_key, w_value=w_value, w_out=w_out, norm_ffn=norm_ffn, gate_vector=gate_vector, dense_gate=dense_gate, dense_up=dense_up, dense_down=dense_down, exp_gate=exp_gate, exp_up=exp_up, exp_down=exp_down, routes=routes, route_w=route_w)


epsilon = 1e-06

def reference(tokens, state, norm_mix, w_query, w_key, w_value, w_out, norm_ffn, gate_vector, dense_gate, dense_up, dense_down, exp_gate, exp_up, exp_down, routes, route_w):
    highest = lax.Precision.HIGHEST
    tok_f = tokens.astype(jnp.float32)
    normed = (tok_f * lax.rsqrt(lax.optimization_barrier(jnp.mean(tok_f * tok_f, axis=1, keepdims=True)) + epsilon) * norm_mix).astype(jnp.bfloat16)
    query = jnp.dot(normed, w_query, preferred_element_type=jnp.float32).astype(jnp.bfloat16)
    key_rows = jnp.dot(normed, w_key, preferred_element_type=jnp.float32).astype(jnp.bfloat16)
    value_rows = jnp.dot(normed, w_value, preferred_element_type=jnp.float32).astype(jnp.bfloat16)
    row_count = tokens.shape[0]
    query3 = query.astype(jnp.float32).reshape(row_count, HEADS, HEAD)
    key3 = key_rows.astype(jnp.float32).reshape(row_count, HEADS, HEAD) * HEAD ** (-0.5)
    value3 = value_rows.astype(jnp.float32).reshape(row_count, HEADS, HEAD)
    head_ids = jnp.arange(HEADS, dtype=jnp.float32)
    decay = 1.0 - jnp.exp2(-3.0 - 2.0 * head_ids)
    new_state = decay[None, :, None, None] * state + jnp.einsum('shd,she->shde', key3, value3, precision=highest)
    read = jnp.einsum('shd,shde->she', query3, new_state, precision=highest)
    centre = lax.optimization_barrier(jnp.mean(read, axis=2, keepdims=True))
    spread = lax.optimization_barrier(jnp.mean(jnp.square(read - centre), axis=2, keepdims=True))
    heads_out = ((read - centre) * lax.rsqrt(spread + epsilon)).astype(jnp.bfloat16).reshape(row_count, HEADS * HEAD)
    group_cols = HEADS * HEAD // N_TP
    mix_sum = jnp.zeros((row_count, D), jnp.float32)
    for group in range(N_TP):
        lower = group * group_cols
        partial_value = jnp.dot(heads_out[:, lower:lower + group_cols], w_out[lower:lower + group_cols], preferred_element_type=jnp.float32)
        rounded = lax.optimization_barrier(partial_value.astype(jnp.bfloat16))
        mix_sum = mix_sum + rounded.astype(jnp.float32)
    after = (tok_f + mix_sum).astype(jnp.bfloat16)
    after_f = after.astype(jnp.float32)
    normed2 = (after_f * lax.rsqrt(lax.optimization_barrier(jnp.mean(after_f * after_f, axis=1, keepdims=True)) + epsilon) * norm_ffn).astype(jnp.bfloat16)
    dense_pre = jnp.dot(normed2, dense_gate, preferred_element_type=jnp.float32)
    up_pre = jnp.dot(normed2, dense_up, preferred_element_type=jnp.float32)
    logit = jnp.dot(normed2, gate_vector, preferred_element_type=jnp.float32)
    dense_hidden = (jax.nn.sigmoid(logit)[:, None] * jax.nn.silu(dense_pre) * up_pre).astype(jnp.bfloat16)
    dense = jnp.dot(dense_hidden, dense_down, preferred_element_type=jnp.float32)
    group_size = N_EP // EXPERTS
    part_ff = exp_gate.shape[2]
    gate_all = exp_gate.reshape(EXPERTS, group_size, D, part_ff).transpose(0, 2, 1, 3).reshape(EXPERTS, D, group_size * part_ff)
    up_all = exp_up.reshape(EXPERTS, group_size, D, part_ff).transpose(0, 2, 1, 3).reshape(EXPERTS, D, group_size * part_ff)
    down_all = exp_down.reshape(EXPERTS, group_size * part_ff, D)
    onehot = (routes[:, :, None] == jnp.arange(EXPERTS, dtype=jnp.int32)[None, None, :]).astype(jnp.float32)
    member = lax.optimization_barrier(jnp.sum(onehot, axis=1))
    weight = lax.optimization_barrier(jnp.sum(onehot * route_w.astype(jnp.float32)[:, :, None], axis=1))
    member_b = member.reshape(N_EP, SEQ_DEV, EXPERTS)
    slot_b = jnp.cumsum(member_b, axis=1) - member_b
    weight_b = weight.reshape(N_EP, SEQ_DEV, EXPERTS)
    rows_b = normed2.astype(jnp.float32).reshape(N_EP, SEQ_DEV, D)
    slot_ids = jnp.arange(CAP, dtype=jnp.float32)

    def one_expert(total, inputs):
        gate_w, up_w, down_w, pick, place, scale = inputs
        select = pick[:, None, :] * (place[:, None, :] == slot_ids[None, :, None]).astype(jnp.float32)
        chosen = jnp.einsum('ncr,nrd->ncd', select, rows_b, precision=highest).astype(jnp.bfloat16).reshape(N_EP * CAP, D)
        gate_pre = jnp.dot(chosen, gate_w, preferred_element_type=jnp.float32)
        up_part = jnp.dot(chosen, up_w, preferred_element_type=jnp.float32)
        hidden = (jax.nn.silu(gate_pre) * up_part).astype(jnp.bfloat16)
        result = jnp.dot(hidden, down_w, preferred_element_type=jnp.float32).reshape(N_EP, CAP, D)
        contrib = jnp.einsum('ncr,ncd->nrd', select * scale[:, None, :], result, precision=highest)
        return (total + contrib, None)
    moe, _ = lax.scan(one_expert, jnp.zeros((N_EP, SEQ_DEV, D), jnp.float32), (gate_all, up_all, down_all, member_b.transpose(2, 0, 1), slot_b.transpose(2, 0, 1), weight_b.transpose(2, 0, 1)))
    mixed = (after_f + moe.reshape(row_count, D) + dense).astype(jnp.bfloat16)
    return (mixed, new_state)
```

```python
import jax
import jax.numpy as jnp
from jax import lax
from jax.sharding import Mesh
from jax.sharding import PartitionSpec as P


EXPERTS = 8
SLOTS = 3
EP = ("ep_0", "ep_1", "ep_2")
PLANE = ("ep_1", "ep_2")
PAD = 24

epsilon = 1e-06
F32 = jnp.float32
BF16 = jnp.bfloat16


def swap(value):
    return lax.ppermute(value, "tp", [(0, 1), (1, 0)])


def along_z(value, shift):
    size = lax.axis_size("ep_0")
    return lax.ppermute(value, "ep_0", [(i, (i + shift) % size) for i in range(size)])


def dot(a, b):
    return jnp.dot(a, b, preferred_element_type=F32)


def dot_t(a, b):
    return lax.dot_general(a, b, (((1,), (1,)), ((), ())), preferred_element_type=F32)


def in_order(core, own, other, dim):
    return jnp.where(
        core == 0,
        jnp.concatenate([own, other], axis=dim),
        jnp.concatenate([other, own], axis=dim),
    )


def silu(v):
    return v / (1.0 + jnp.exp(-v))


def body(
    tokens,
    state,
    norm_mix,
    w_query,
    w_key,
    w_value,
    w_out,
    norm_ffn,
    gate_vector,
    dense_gate,
    dense_up,
    dense_down,
    exp_gate,
    exp_up,
    exp_down,
    routes,
    route_w,
):
    core = lax.axis_index("tp")
    rows, half = tokens.shape
    heads, head = state.shape[1], state.shape[2]
    width = 2 * half
    hidden = dense_gate.shape[1]

    full_x = in_order(core, tokens, swap(tokens), 1)

    vectors = jnp.stack([norm_ffn, gate_vector.astype(F32)])
    vectors = in_order(core, vectors, swap(vectors), 1)
    gain, gate_full = vectors[0], vectors[1].astype(BF16)
    fill = jnp.zeros((PAD - hidden, half), BF16)
    packed = jnp.concatenate(
        [dense_gate.T, fill, dense_up.T, fill, dense_down, fill], axis=0
    )[None]
    near = jnp.concatenate([along_z(packed, 1), packed, along_z(packed, -1)], axis=0)
    dense_own = jnp.concatenate([along_z(near, 3), near, along_z(near[:2], -3)], axis=0)
    dense_other = swap(dense_own)
    gate2, up2, down2 = swap(exp_gate[0]), swap(exp_up[0]), swap(exp_down[0])

    full_f = full_x.astype(F32)
    normed = (
        full_f
        * lax.rsqrt(jnp.sum(full_f * full_f, axis=1, keepdims=True) / width + epsilon)
        * norm_mix
    ).astype(BF16)
    query = dot(normed, w_query).astype(BF16)
    key_rows = dot(normed, w_key).astype(BF16)
    value_rows = dot(normed, w_value).astype(BF16)
    query3 = query.astype(F32).reshape(rows, heads, head)
    key3 = key_rows.astype(F32).reshape(rows, heads, head) * head ** (-0.5)
    value3 = value_rows.astype(F32).reshape(rows, heads, head)
    head_ids = (core * heads + jnp.arange(heads, dtype=jnp.int32)).astype(F32)
    decay = 1.0 - jnp.exp2(-3.0 - 2.0 * head_ids)
    new_state = decay[None, :, None, None] * state + jnp.einsum("shd,she->shde", key3, value3)
    read = jnp.einsum("shd,shde->she", query3, new_state)
    centre = jnp.mean(read, axis=2, keepdims=True)
    spread = jnp.mean(jnp.square(read - centre), axis=2, keepdims=True)
    heads_out = (
        ((read - centre) * lax.rsqrt(spread + epsilon)).astype(BF16).reshape(rows, heads * head)
    )
    mix_part = dot(heads_out, w_out).astype(BF16)
    mix_sum = mix_part.astype(F32) + swap(mix_part).astype(F32)
    after = (full_f + mix_sum).astype(BF16)
    after_f = after.astype(F32)
    squares = jnp.sum(after_f * after_f, axis=1, keepdims=True)
    normed2 = (after_f * lax.rsqrt(squares / width + epsilon) * gain).astype(BF16)

    ids = jnp.arange(EXPERTS, dtype=jnp.int32)
    chosen = (routes[:, :, None] == ids[None, None, :]).astype(F32)
    member = jnp.sum(chosen, axis=1)
    weight = jnp.sum(chosen * route_w.astype(F32)[:, :, None], axis=1)
    before = jnp.tril(jnp.ones((rows, rows), F32), -1)
    place = dot(before, member)
    slot_ids = jnp.arange(2 * SLOTS, dtype=F32)
    select = member.T[:, None, :] * (place.T[:, None, :] == slot_ids[None, :, None]).astype(F32)
    mine = lax.dynamic_slice_in_dim(select, core * SLOTS, SLOTS, 1)
    slot_w = jnp.sum(mine * weight.T[:, None, :], axis=2).reshape(EXPERTS * SLOTS, 1)
    slot_x = dot(mine.reshape(EXPERTS * SLOTS, rows).astype(BF16), normed2).astype(BF16)
    slot_rows = jnp.concatenate(
        [slot_x, jnp.broadcast_to(slot_w.astype(BF16), (EXPERTS * SLOTS, 128))], axis=1
    )
    at_plane = lax.all_to_all(
        slot_rows.reshape(EXPERTS, SLOTS, width + 128), "ep_0", 0, 0, tiled=True
    ).reshape(1, EXPERTS * SLOTS, width + 128)
    chips = lax.axis_size(PLANE)
    gathered = lax.all_to_all(
        jnp.broadcast_to(at_plane, (chips, *at_plane.shape[1:])), PLANE, 0, 0, tiled=True
    ).reshape(chips * EXPERTS * SLOTS, width + 128)

    x = gathered[:, :width]
    w = gathered[:, width : width + 1].astype(F32)
    h1 = (w * silu(dot(x, exp_gate[0])) * dot(x, exp_up[0])).astype(BF16)
    h2 = (w * silu(dot(x, gate2)) * dot(x, up2)).astype(BF16)
    partial = dot(h1, exp_down[0]) + dot(h2, down2)
    lead = dense_own.shape[0] * PAD
    dense_full = in_order(core, dense_own, dense_other, 2)
    gate_d = dense_full[:, :PAD].reshape(lead, width)
    up_d = dense_full[:, PAD : 2 * PAD].reshape(lead, width)
    down_d = dense_full[:, 2 * PAD :].reshape(lead, width)
    logit = dot(x, gate_full)
    hd = (0.5 * jax.nn.sigmoid(logit)[:, None] * silu(dot_t(x, gate_d)) * dot_t(x, up_d)).astype(
        BF16
    )
    partial = (partial + dot(hd, down_d)).astype(BF16)

    back = lax.all_to_all(
        partial.reshape(chips, EXPERTS * SLOTS, width), PLANE, 0, 0, tiled=True
    )
    summed = jnp.sum(back.astype(F32), axis=0).astype(BF16)
    send = summed.reshape(EXPERTS, SLOTS, 2, half).transpose(0, 2, 1, 3)
    home = lax.all_to_all(
        send.reshape(2 * EXPERTS, SLOTS, half), ("ep_0", "tp"), 0, 0, tiled=True
    ).reshape(2 * EXPERTS * SLOTS, half)
    combine = select.reshape(EXPERTS * 2 * SLOTS, rows).astype(BF16)
    combined = lax.dot_general(
        combine, home, (((0,), (0,)), ((), ())), preferred_element_type=F32
    )
    after_half = lax.dynamic_slice_in_dim(after, core * half, half, 1)
    return ((after_half.astype(F32) + combined).astype(BF16), new_state)


def solution(mesh):
    finer = Mesh(mesh.devices.reshape(8, 4, 4, mesh.shape["tp"]), ("ep_0", "ep_1", "ep_2", "tp"))
    in_specs = (
        P(EP, "tp"),
        P(EP, "tp", None, None),
        P(),
        P(None, "tp"),
        P(None, "tp"),
        P(None, "tp"),
        P("tp", None),
        P("tp"),
        P("tp"),
        P("tp", EP),
        P("tp", EP),
        P(EP, "tp"),
        P(EP, None, "tp"),
        P(EP, None, "tp"),
        P(EP, "tp", None),
        P(EP, None),
        P(EP, None),
    )
    out_specs = (P(EP, "tp"), P(EP, "tp", None, None))
    return jax.shard_map(body, mesh=finer, in_specs=in_specs, out_specs=out_specs, check_vma=False)
```

```python
import jax
import jax.numpy as jnp
from jax import lax
from jax.experimental import pallas as pl
from jax.experimental.pallas import tpu as pltpu
from jax.sharding import Mesh
from jax.sharding import PartitionSpec as P


EXPERTS = 8
SLOTS = 3
EP = ("ep_0", "ep_1", "ep_2")
PLANE = ("ep_1", "ep_2")
PAD = 24
CHUNK = 80

epsilon = 1e-06
F32 = jnp.float32
BF16 = jnp.bfloat16


def swap(value):
    return lax.ppermute(value, "tp", [(0, 1), (1, 0)])


def along_z(value, shift):
    size = lax.axis_size("ep_0")
    return lax.ppermute(value, "ep_0", [(i, (i + shift) % size) for i in range(size)])


def to_all(value, axis):
    size = lax.axis_size(axis)
    copies = jnp.broadcast_to(value[None], (size, *value.shape))
    return lax.all_to_all(copies, axis, split_axis=0, concat_axis=0, tiled=True)


def dot(a, b):
    return jnp.dot(a, b, preferred_element_type=F32)


def dot_t(a, b):
    return lax.dot_general(a, b, (((1,), (1,)), ((), ())), preferred_element_type=F32)


def silu(v):
    return v / (1.0 + jnp.exp(-v))


def branch_kernel(
    hidden, core_ref, x_ref, g1, u1, d1, g2, u2, d2, own_ref, other_ref, out_ref, acc_ref
):
    half = own_ref.shape[1]
    width = 2 * half
    core = core_ref[0]
    here = pl.multiple_of(core * half, half)
    there = pl.multiple_of((1 - core) * half, half)
    total = x_ref.shape[0]
    step = total // 3
    for start in range(0, total, step):
        band = pl.ds(start, step)
        x = x_ref[band, :width]
        w = x_ref[band, width : width + 1].astype(F32)
        h1 = (w * silu(dot_t(x, g1[...])) * dot_t(x, u1[...])).astype(BF16)
        h2 = (w * silu(dot_t(x, g2[...])) * dot_t(x, u2[...])).astype(BF16)
        acc_ref[...] = dot(h1, d1[...]) + dot(h2, d2[...])
        pre = dot_t(x_ref[band, pl.ds(here, half)], own_ref[...])
        pre = pre + dot_t(x_ref[band, pl.ds(there, half)], other_ref[...])
        logit = pre[:, hidden : hidden + 1]
        gate = pltpu.roll(pre, 2 * PAD, 1)
        up = pltpu.roll(pre, PAD, 1)
        unit = lax.broadcasted_iota(jnp.int32, pre.shape, 1) % CHUNK
        live = (unit >= 2 * PAD) & (unit < 2 * PAD + hidden)
        scale = 0.5 / (1.0 + jnp.exp(-logit))
        hd = jnp.where(live, scale * silu(gate) * up, 0.0).astype(BF16)
        acc_ref[:, pl.ds(here, half)] += dot(hd, own_ref[...])
        acc_ref[:, pl.ds(there, half)] += dot(hd, other_ref[...])
        out_ref[band, :] = acc_ref[...].astype(BF16)


def experts_and_dense(core, x, own, other, dense_own, dense_other, hidden):
    rows, width = x.shape[0], 2 * dense_own.shape[1]
    vmem = pl.BlockSpec(memory_space=pltpu.VMEM)
    return pl.pallas_call(
        lambda *refs: branch_kernel(hidden, *refs),
        name="branch",
        out_shape=jax.ShapeDtypeStruct((rows, width), BF16),
        in_specs=[pl.BlockSpec(memory_space=pltpu.SMEM)] + [vmem] * 9,
        out_specs=vmem,
        scratch_shapes=[pltpu.VMEM((rows // 3, width), F32)],
    )(core.reshape(1), x, *own, *other, dense_own, dense_other)


def mixer_kernel(
    core_ref, x_ref, y_ref, gain_ref, wq, wk, wv, wo, state_ref, mix_ref, new_hbm,
    new_ref, turn_ref, read_ref, sem,
):
    rows, half = x_ref.shape
    heads, head = state_ref.shape[1], state_ref.shape[2]
    core = core_ref[0]
    here = pl.multiple_of(core * half, half)
    there = pl.multiple_of((1 - core) * half, half)
    x = x_ref[...].astype(F32)
    y = y_ref[...].astype(F32)
    total = jnp.sum(x * x, axis=1, keepdims=True) + jnp.sum(y * y, axis=1, keepdims=True)
    scale = lax.rsqrt(total / (2 * half) + epsilon)
    x = (x * scale * gain_ref[:, pl.ds(here, half)]).astype(BF16)
    y = (y * scale * gain_ref[:, pl.ds(there, half)]).astype(BF16)

    def project(ref):
        both = dot(x, ref[pl.ds(here, half), :]) + dot(y, ref[pl.ds(there, half), :])
        return both.astype(BF16).astype(F32)

    query = project(wq)
    key = project(wk) * head ** (-0.5)
    value = project(wv)
    turn_ref[0] = query.T
    turn_ref[1] = key.T
    decays = [
        jnp.where(core == 0, 1.0 - 2.0 ** (-3 - 2 * h), 1.0 - 2.0 ** (-3 - 2 * (h + heads)))
        for h in range(heads)
    ]
    group = 4
    copies = []
    for s in range(rows):
        for h in range(heads):
            part = slice(h * head, (h + 1) * head)
            q = turn_ref[0, part, s : s + 1]
            k = turn_ref[1, part, s : s + 1]
            new = decays[h] * state_ref[s, h] + k * value[s : s + 1, part]
            new_ref[s, h] = new
            read_ref[s : s + 1, part] = jnp.sum(q * new, axis=0, keepdims=True)
        if s % group == group - 1:
            band = pl.ds(s + 1 - group, group)
            copy = pltpu.make_async_copy(new_ref.at[band], new_hbm.at[band], sem.at[s // group])
            copy.start()
            copies.append(copy)
    outs = []
    for h in range(heads):
        read = read_ref[:, h * head : (h + 1) * head]
        centre = jnp.mean(read, axis=1, keepdims=True)
        spread = jnp.mean(jnp.square(read - centre), axis=1, keepdims=True)
        outs.append(((read - centre) * lax.rsqrt(spread + epsilon)).astype(BF16))
    mix = jnp.zeros(mix_ref.shape, F32)
    for h in range(heads):
        mix = mix + dot(outs[h], wo[h * head : (h + 1) * head, :])
    mix_ref[...] = mix.astype(BF16)
    for copy in copies:
        copy.wait()


def mixer(core, own, other, gain, wq, wk, wv, wo, state):
    rows, half = own.shape
    heads, head = state.shape[1], state.shape[2]
    vmem = pl.BlockSpec(memory_space=pltpu.VMEM)
    return pl.pallas_call(
        mixer_kernel,
        name="mixer",
        out_shape=(
            jax.ShapeDtypeStruct((rows, 2 * half), BF16),
            jax.ShapeDtypeStruct(state.shape, F32),
        ),
        in_specs=[pl.BlockSpec(memory_space=pltpu.SMEM)] + [vmem] * 8,
        out_specs=(vmem, pl.BlockSpec(memory_space=pl.ANY)),
        scratch_shapes=[
            pltpu.VMEM(state.shape, F32),
            pltpu.VMEM((2, heads * head, rows), F32),
            pltpu.VMEM((rows, heads * head), F32),
            pltpu.SemaphoreType.DMA((rows // 4,)),
        ],
    )(core.reshape(1), own, other, gain.reshape(1, 2 * half), wq, wk, wv, wo, state)


def third(index):
    return (index * 11) >> 5


def slots_kernel(
    core_ref, x_ref, y_ref, mix_ref, mix2_ref, gain_ref, gain2_ref, routes_ref, weights_ref,
    slot_ref, after_ref,
):
    rows, half = x_ref.shape
    core = core_ref[0]
    here = pl.multiple_of(core * half, half)
    there = pl.multiple_of((1 - core) * half, half)

    def add(ref, at):
        total = mix_ref[:, pl.ds(at, half)].astype(F32) + mix2_ref[:, pl.ds(at, half)].astype(F32)
        return (ref[...].astype(F32) + total).astype(BF16)

    after = add(x_ref, here)
    after_ref[...] = after
    x = after.astype(F32)
    y = add(y_ref, there).astype(F32)
    total = jnp.sum(x * x, axis=1, keepdims=True) + jnp.sum(y * y, axis=1, keepdims=True)
    scale = lax.rsqrt(total / (2 * half) + epsilon)
    x = (x * scale * gain_ref[...]).astype(BF16)
    y = (y * scale * gain2_ref[...]).astype(BF16)

    shape = (EXPERTS * SLOTS, rows)
    slot = lax.broadcasted_iota(jnp.int32, shape, 0)
    expert = third(slot)
    slot = slot - SLOTS * expert + SLOTS * core
    first = (routes_ref[0:1, :] == expert).astype(F32)
    second = (routes_ref[1:2, :] == expert).astype(F32)
    member = first + second
    earlier = lax.broadcasted_iota(jnp.int32, (rows, rows), 0) < lax.broadcasted_iota(
        jnp.int32, (rows, rows), 1
    )
    place = dot(member.astype(BF16), earlier.astype(F32).astype(BF16))
    select = jnp.where(place == slot.astype(F32), member, 0.0)
    weight = first * weights_ref[0:1, :].astype(F32) + second * weights_ref[1:2, :].astype(F32)
    weight = jnp.sum(select * weight, axis=1, keepdims=True)
    select = select.astype(BF16)
    slot_ref[:, pl.ds(here, half)] = dot(select, x).astype(BF16)
    slot_ref[:, pl.ds(there, half)] = dot(select, y).astype(BF16)
    slot_ref[:, 2 * half :] = jnp.broadcast_to(weight, (EXPERTS * SLOTS, 128)).astype(BF16)


def to_slots(core, own, other, mix, mix2, gain, gain2, routes, route_w):
    rows, half = own.shape
    vmem = pl.BlockSpec(memory_space=pltpu.VMEM)
    return pl.pallas_call(
        slots_kernel,
        name="slots",
        out_shape=(
            jax.ShapeDtypeStruct((EXPERTS * SLOTS, 2 * half + 128), BF16),
            jax.ShapeDtypeStruct((rows, half), BF16),
        ),
        in_specs=[pl.BlockSpec(memory_space=pltpu.SMEM)] + [vmem] * 8,
        out_specs=(vmem, vmem),
    )(
        core.reshape(1), own, other, mix, mix2, gain.reshape(1, half), gain2.reshape(1, half),
        routes.T, route_w.astype(F32).T,
    )


def home_kernel(home_ref, after_ref, routes_ref, out_ref):
    rows = after_ref.shape[0]
    shape = (rows, home_ref.shape[0])
    slot = lax.broadcasted_iota(jnp.int32, shape, 1)
    expert = third(slot >> 1)
    slot = slot - 2 * SLOTS * expert
    member = (routes_ref[:, 0:1] == expert).astype(F32) + (routes_ref[:, 1:2] == expert).astype(F32)
    earlier = lax.broadcasted_iota(jnp.int32, (rows, rows), 1) < lax.broadcasted_iota(
        jnp.int32, (rows, rows), 0
    )
    place = dot(earlier.astype(F32).astype(BF16), member.astype(BF16))
    select = jnp.where(place == slot.astype(F32), member, 0.0).astype(BF16)
    total = after_ref[...].astype(F32) + dot(select, home_ref[...])
    out_ref[...] = total.astype(BF16)


def at_home(home, after, routes):
    vmem = pl.BlockSpec(memory_space=pltpu.VMEM)
    return pl.pallas_call(
        home_kernel,
        name="home",
        out_shape=jax.ShapeDtypeStruct(after.shape, BF16),
        in_specs=[vmem] * 3,
        out_specs=vmem,
    )(home, after, routes)


def layer(
    tokens, state, norm_mix, w_query, w_key, w_value, w_out, norm_ffn, gate_vector,
    dense_gate, dense_up, dense_down, exp_gate, exp_up, exp_down, routes, route_w,
):
    core = lax.axis_index("tp")
    half = tokens.shape[1]
    width = 2 * half
    hidden = dense_gate.shape[1]

    def fill(size):
        return jnp.zeros((size, half), BF16)

    other_x = swap(tokens)
    other_gain = swap(norm_ffn)
    packed = jnp.concatenate(
        [
            dense_gate.T,
            gate_vector[None],
            fill(PAD - hidden - 1),
            dense_up.T,
            fill(PAD - hidden),
            dense_down,
            fill(CHUNK - 2 * PAD - hidden),
        ],
        axis=0,
    )
    mine = (exp_gate[0].T, exp_up[0].T, exp_down[0])
    theirs = tuple(swap(weights) for weights in mine)

    mix, new_state = mixer(core, tokens, other_x, norm_mix, w_query, w_key, w_value, w_out, state)
    mix2 = swap(mix)
    slot_rows, after = to_slots(
        core, tokens, other_x, mix, mix2, norm_ffn, other_gain, routes, route_w
    )
    at_plane = lax.all_to_all(
        slot_rows.reshape(EXPERTS, SLOTS, width + 128), "ep_0", 0, 0, tiled=True
    ).reshape(EXPERTS * SLOTS, width + 128)
    pieces = [packed] + [along_z(packed, k) for k in range(1, EXPERTS)]
    dense_own = jnp.concatenate(pieces, axis=0)
    dense_other = swap(dense_own)
    gathered = to_all(at_plane, PLANE)
    chips = gathered.shape[0]
    partial = experts_and_dense(
        core,
        gathered.reshape(-1, width + 128),
        mine,
        theirs,
        dense_own,
        dense_other,
        hidden,
    )
    back = lax.all_to_all(partial.reshape(chips, EXPERTS * SLOTS, width), PLANE, 0, 0, tiled=True)
    summed = jnp.sum(back.astype(F32), axis=0).astype(BF16)
    send = summed.reshape(EXPERTS, SLOTS, 2, half).transpose(0, 2, 1, 3)
    home = lax.all_to_all(
        send.reshape(2 * EXPERTS, SLOTS, half), ("ep_0", "tp"), 0, 0, tiled=True
    ).reshape(2 * EXPERTS * SLOTS, half)
    return (at_home(home, after, routes), new_state)


def solution(mesh):
    finer = Mesh(mesh.devices.reshape(8, 4, 4, mesh.shape["tp"]), ("ep_0", "ep_1", "ep_2", "tp"))
    in_specs = (
        P(EP, "tp"),
        P(EP, "tp", None, None),
        P(),
        P(None, "tp"),
        P(None, "tp"),
        P(None, "tp"),
        P("tp", None),
        P("tp"),
        P("tp"),
        P("tp", EP),
        P("tp", EP),
        P(EP, "tp"),
        P(EP, None, "tp"),
        P(EP, None, "tp"),
        P(EP, "tp", None),
        P(EP, None),
        P(EP, None),
    )
    out_specs = (P(EP, "tp"), P(EP, "tp", None, None))
    return jax.shard_map(layer, mesh=finer, in_specs=in_specs, out_specs=out_specs, check_vma=False)
```

```python
import jax
import jax.numpy as jnp
from jax import lax
from jax.experimental import pallas as pl
from jax.experimental.pallas import tpu as pltpu
from jax.sharding import Mesh
from jax.sharding import PartitionSpec as P


EXPERTS = 8
SLOTS = 3
EP = ("ep_0", "ep_1", "ep_2")
PLANE = ("ep_1", "ep_2")
PAD = 24
CHUNK = 80

epsilon = 1e-06
F32 = jnp.float32
BF16 = jnp.bfloat16


def swap(value):
    return lax.ppermute(value, "tp", [(0, 1), (1, 0)])


def along_z(value, shift):
    size = lax.axis_size("ep_0")
    return lax.ppermute(value, "ep_0", [(i, (i + shift) % size) for i in range(size)])


def to_all(value, axis):
    size = lax.axis_size(axis)
    copies = jnp.broadcast_to(value[None], (size, *value.shape))
    return lax.all_to_all(copies, axis, split_axis=0, concat_axis=0, tiled=True)


def dot(a, b):
    return jnp.dot(a, b, preferred_element_type=F32)


def dot_t(a, b):
    return lax.dot_general(a, b, (((1,), (1,)), ((), ())), preferred_element_type=F32)


def silu(v):
    return v / (1.0 + jnp.exp(-v))


def branch_kernel(hidden, core_ref, x_ref, *refs):
    weights, pieces, (out_ref, w_ref, own_ref, other_ref, acc_ref, sem) = (
        refs[:6], refs[6:-6], refs[-6:],
    )
    half = own_ref.shape[1]
    width = 2 * half
    count = len(pieces) // 2
    first = []
    for k, weight in enumerate(weights):
        first.append(pltpu.make_async_copy(weight, w_ref.at[k], sem.at[len(pieces) + k]))
        first[-1].start()
    copies = []
    for k, piece in enumerate(pieces):
        into = (own_ref, other_ref)[k // count]
        place = pl.ds((k % count) * CHUNK, CHUNK)
        copies.append(pltpu.make_async_copy(piece, into.at[place], sem.at[k]))
        copies[-1].start()
    core = core_ref[0]
    here = pl.multiple_of(core * half, half)
    there = pl.multiple_of((1 - core) * half, half)
    total = x_ref.shape[0]
    step = total // 3
    for copy in first:
        copy.wait()
    g1, u1, d1, g2, u2, d2 = (w_ref.at[k] for k in range(6))
    for start in range(0, total, step):
        band = pl.ds(start, step)
        x = x_ref[band, :width]
        w = x_ref[band, width : width + 1].astype(F32)
        h1 = (w * silu(dot_t(x, g1[...])) * dot_t(x, u1[...])).astype(BF16)
        h2 = (w * silu(dot_t(x, g2[...])) * dot_t(x, u2[...])).astype(BF16)
        acc_ref[...] = dot(h1, d1[...]) + dot(h2, d2[...])
        if start == 0:
            for copy in copies:
                copy.wait()
        pre = dot_t(x_ref[band, pl.ds(here, half)], own_ref[...])
        pre = pre + dot_t(x_ref[band, pl.ds(there, half)], other_ref[...])
        logit = pre[:, hidden : hidden + 1]
        gate = pltpu.roll(pre, 2 * PAD, 1)
        up = pltpu.roll(pre, PAD, 1)
        unit = lax.broadcasted_iota(jnp.int32, pre.shape, 1) % CHUNK
        live = (unit >= 2 * PAD) & (unit < 2 * PAD + hidden)
        scale = 0.5 / (1.0 + jnp.exp(-logit))
        hd = jnp.where(live, scale * silu(gate) * up, 0.0).astype(BF16)
        acc_ref[:, pl.ds(here, half)] += dot(hd, own_ref[...])
        acc_ref[:, pl.ds(there, half)] += dot(hd, other_ref[...])
        out_ref[band, :] = acc_ref[...].astype(BF16)


def in_vmem(value):
    return pltpu.with_memory_space_constraint(value, pltpu.VMEM)


def experts_and_dense(core, x, own, other, pieces, pieces2, hidden):
    rows, half = x.shape[0], pieces[0].shape[1]
    width = 2 * half
    vmem = pl.BlockSpec(memory_space=pltpu.VMEM)
    hbm = pl.BlockSpec(memory_space=pl.ANY)
    units = len(pieces) * CHUNK
    return pl.pallas_call(
        lambda *refs: branch_kernel(hidden, *refs),
        name="branch",
        out_shape=pltpu.VMEM((rows, width), BF16),
        in_specs=[pl.BlockSpec(memory_space=pltpu.SMEM)] + [vmem] + [hbm] * (6 + 2 * len(pieces)),
        out_specs=vmem,
        scratch_shapes=[
            pltpu.VMEM((6, *own[0].shape), BF16),
            pltpu.VMEM((units, half), BF16),
            pltpu.VMEM((units, half), BF16),
            pltpu.VMEM((rows // 3, width), F32),
            pltpu.SemaphoreType.DMA((6 + 2 * len(pieces),)),
        ],
    )(core.reshape(1), in_vmem(x), *own, *other, *pieces, *pieces2)


def mixer_kernel(
    core_ref, x_ref, y_ref, gain_ref, wq, wk, wv, wo, state_ref, mix_ref, new_hbm,
    new_ref, turn_ref, read_ref, sem,
):
    rows, half = x_ref.shape
    heads, head = state_ref.shape[1], state_ref.shape[2]
    core = core_ref[0]
    here = pl.multiple_of(core * half, half)
    there = pl.multiple_of((1 - core) * half, half)
    x = x_ref[...].astype(F32)
    y = y_ref[...].astype(F32)
    total = jnp.sum(x * x, axis=1, keepdims=True) + jnp.sum(y * y, axis=1, keepdims=True)
    scale = lax.rsqrt(total / (2 * half) + epsilon)
    x = (x * scale * gain_ref[:, pl.ds(here, half)]).astype(BF16)
    y = (y * scale * gain_ref[:, pl.ds(there, half)]).astype(BF16)

    def project(ref):
        both = dot(x, ref[pl.ds(here, half), :]) + dot(y, ref[pl.ds(there, half), :])
        return both.astype(BF16).astype(F32)

    query = project(wq)
    key = project(wk) * head ** (-0.5)
    value = project(wv)
    turn_ref[0] = query.T
    turn_ref[1] = key.T
    decays = [
        jnp.where(core == 0, 1.0 - 2.0 ** (-3 - 2 * h), 1.0 - 2.0 ** (-3 - 2 * (h + heads)))
        for h in range(heads)
    ]
    group = 4
    copies = []
    for s in range(rows):
        for h in range(heads):
            part = slice(h * head, (h + 1) * head)
            q = turn_ref[0, part, s : s + 1]
            k = turn_ref[1, part, s : s + 1]
            new = decays[h] * state_ref[s, h] + k * value[s : s + 1, part]
            new_ref[s, h] = new
            read_ref[s : s + 1, part] = jnp.sum(q * new, axis=0, keepdims=True)
        if s % group == group - 1:
            band = pl.ds(s + 1 - group, group)
            copy = pltpu.make_async_copy(new_ref.at[band], new_hbm.at[band], sem.at[s // group])
            copy.start()
            copies.append(copy)
    outs = []
    for h in range(heads):
        read = read_ref[:, h * head : (h + 1) * head]
        centre = jnp.mean(read, axis=1, keepdims=True)
        spread = jnp.mean(jnp.square(read - centre), axis=1, keepdims=True)
        outs.append(((read - centre) * lax.rsqrt(spread + epsilon)).astype(BF16))
    mix = jnp.zeros(mix_ref.shape, F32)
    for h in range(heads):
        mix = mix + dot(outs[h], wo[h * head : (h + 1) * head, :])
    mix_ref[...] = mix.astype(BF16)
    for copy in copies:
        copy.wait()


def mixer(core, own, other, gain, wq, wk, wv, wo, state):
    rows, half = own.shape
    heads, head = state.shape[1], state.shape[2]
    vmem = pl.BlockSpec(memory_space=pltpu.VMEM)
    return pl.pallas_call(
        mixer_kernel,
        name="mixer",
        out_shape=(
            pltpu.VMEM((rows, 2 * half), BF16),
            jax.ShapeDtypeStruct(state.shape, F32),
        ),
        in_specs=[pl.BlockSpec(memory_space=pltpu.SMEM)] + [vmem] * 8,
        out_specs=(vmem, pl.BlockSpec(memory_space=pl.ANY)),
        scratch_shapes=[
            pltpu.VMEM(state.shape, F32),
            pltpu.VMEM((2, heads * head, rows), F32),
            pltpu.VMEM((rows, heads * head), F32),
            pltpu.SemaphoreType.DMA((rows // 4,)),
        ],
    )(
        core.reshape(1), in_vmem(own), in_vmem(other), gain.reshape(1, 2 * half),
        wq, wk, wv, wo, state,
    )


def third(index):
    return (index * 11) >> 5


def slots_kernel(
    core_ref, x_ref, y_ref, mix_ref, mix2_ref, gain_ref, gain2_ref, routes_ref, weights_ref,
    slot_ref, after_ref,
):
    rows, half = x_ref.shape
    core = core_ref[0]
    here = pl.multiple_of(core * half, half)
    there = pl.multiple_of((1 - core) * half, half)

    def add(ref, at):
        total = mix_ref[:, pl.ds(at, half)].astype(F32) + mix2_ref[:, pl.ds(at, half)].astype(F32)
        return (ref[...].astype(F32) + total).astype(BF16)

    after = add(x_ref, here)
    after_ref[...] = after
    x = after.astype(F32)
    y = add(y_ref, there).astype(F32)
    total = jnp.sum(x * x, axis=1, keepdims=True) + jnp.sum(y * y, axis=1, keepdims=True)
    scale = lax.rsqrt(total / (2 * half) + epsilon)
    x = (x * scale * gain_ref[...]).astype(BF16)
    y = (y * scale * gain2_ref[...]).astype(BF16)

    shape = (EXPERTS * SLOTS, rows)
    slot = lax.broadcasted_iota(jnp.int32, shape, 0)
    expert = third(slot)
    slot = slot - SLOTS * expert + SLOTS * core
    first = (routes_ref[0:1, :] == expert).astype(F32)
    second = (routes_ref[1:2, :] == expert).astype(F32)
    member = first + second
    earlier = lax.broadcasted_iota(jnp.int32, (rows, rows), 0) < lax.broadcasted_iota(
        jnp.int32, (rows, rows), 1
    )
    place = dot(member.astype(BF16), earlier.astype(F32).astype(BF16))
    select = jnp.where(place == slot.astype(F32), member, 0.0)
    weight = first * weights_ref[0:1, :].astype(F32) + second * weights_ref[1:2, :].astype(F32)
    weight = jnp.sum(select * weight, axis=1, keepdims=True)
    select = select.astype(BF16)
    slot_ref[:, pl.ds(here, half)] = dot(select, x).astype(BF16)
    slot_ref[:, pl.ds(there, half)] = dot(select, y).astype(BF16)
    slot_ref[:, 2 * half :] = jnp.broadcast_to(weight, (EXPERTS * SLOTS, 128)).astype(BF16)


def to_slots(core, own, other, mix, mix2, gain, gain2, routes, route_w):
    rows, half = own.shape
    vmem = pl.BlockSpec(memory_space=pltpu.VMEM)
    return pl.pallas_call(
        slots_kernel,
        name="slots",
        out_shape=(
            pltpu.VMEM((EXPERTS * SLOTS, 2 * half + 128), BF16),
            pltpu.VMEM((rows, half), BF16),
        ),
        in_specs=[pl.BlockSpec(memory_space=pltpu.SMEM)] + [vmem] * 8,
        out_specs=(vmem, vmem),
    )(
        core.reshape(1), in_vmem(own), in_vmem(other), in_vmem(mix), in_vmem(mix2),
        gain.reshape(1, half), in_vmem(gain2.reshape(1, half)), routes.T, route_w.T,
    )


def home_kernel(home_ref, after_ref, routes_ref, out_ref):
    rows = after_ref.shape[0]
    shape = (rows, home_ref.shape[0])
    slot = lax.broadcasted_iota(jnp.int32, shape, 1)
    expert = third(slot >> 1)
    slot = slot - 2 * SLOTS * expert
    member = (routes_ref[:, 0:1] == expert).astype(F32) + (routes_ref[:, 1:2] == expert).astype(F32)
    earlier = lax.broadcasted_iota(jnp.int32, (rows, rows), 1) < lax.broadcasted_iota(
        jnp.int32, (rows, rows), 0
    )
    place = dot(earlier.astype(F32).astype(BF16), member.astype(BF16))
    select = jnp.where(place == slot.astype(F32), member, 0.0).astype(BF16)
    total = after_ref[...].astype(F32) + dot(select, home_ref[...])
    out_ref[...] = total.astype(BF16)


def at_home(home, after, routes):
    vmem = pl.BlockSpec(memory_space=pltpu.VMEM)
    return pl.pallas_call(
        home_kernel,
        name="home",
        out_shape=jax.ShapeDtypeStruct(after.shape, BF16),
        in_specs=[vmem] * 3,
        out_specs=vmem,
    )(in_vmem(home), in_vmem(after), routes)


def layer(
    tokens, state, norm_mix, w_query, w_key, w_value, w_out, norm_ffn, gate_vector,
    dense_gate, dense_up, dense_down, exp_gate, exp_up, exp_down, routes, route_w,
):
    core = lax.axis_index("tp")
    half = tokens.shape[1]
    width = 2 * half
    hidden = dense_gate.shape[1]

    def fill(size):
        return jnp.zeros((size, half), BF16)

    other_x = swap(tokens)
    other_gain = swap(norm_ffn)
    packed = jnp.concatenate(
        [
            dense_gate.T,
            gate_vector[None],
            fill(PAD - hidden - 1),
            dense_up.T,
            fill(PAD - hidden),
            dense_down,
            fill(CHUNK - 2 * PAD - hidden),
        ],
        axis=0,
    )
    mine = (exp_gate[0].T, exp_up[0].T, exp_down[0])
    theirs = tuple(swap(weights) for weights in mine)

    mix, new_state = mixer(core, tokens, other_x, norm_mix, w_query, w_key, w_value, w_out, state)
    mix2 = swap(mix)
    slot_rows, after = to_slots(
        core, tokens, other_x, mix, mix2, norm_ffn, other_gain, routes, route_w
    )
    at_plane = lax.all_to_all(
        slot_rows.reshape(EXPERTS, SLOTS, width + 128), "ep_0", 0, 0, tiled=True
    ).reshape(EXPERTS * SLOTS, width + 128)
    pieces = [packed]
    for shift in (4, 3, 5, 2, 6, 1, 7):
        pieces.append(along_z(packed, shift))
    pieces2 = [swap(piece) for piece in pieces]
    gathered = to_all(at_plane, PLANE)
    chips = gathered.shape[0]
    partial = experts_and_dense(
        core,
        gathered.reshape(-1, width + 128),
        mine,
        theirs,
        pieces,
        pieces2,
        hidden,
    )
    back = lax.all_to_all(partial.reshape(chips, EXPERTS * SLOTS, width), PLANE, 0, 0, tiled=True)
    summed = jnp.sum(back.astype(F32), axis=0).astype(BF16)
    send = summed.reshape(EXPERTS, SLOTS, 2, half).transpose(0, 2, 1, 3)
    home = lax.all_to_all(
        send.reshape(2 * EXPERTS, SLOTS, half), ("ep_0", "tp"), 0, 0, tiled=True
    ).reshape(2 * EXPERTS * SLOTS, half)
    return (at_home(home, after, routes), new_state)


def solution(mesh):
    finer = Mesh(mesh.devices.reshape(8, 4, 4, mesh.shape["tp"]), ("ep_0", "ep_1", "ep_2", "tp"))
    in_specs = (
        P(EP, "tp"),
        P(EP, "tp", None, None),
        P(),
        P(None, "tp"),
        P(None, "tp"),
        P(None, "tp"),
        P("tp", None),
        P("tp"),
        P("tp"),
        P("tp", EP),
        P("tp", EP),
        P(EP, "tp"),
        P(EP, None, "tp"),
        P(EP, None, "tp"),
        P(EP, "tp", None),
        P(EP, None),
        P(EP, None),
    )
    out_specs = (P(EP, "tp"), P(EP, "tp", None, None))
    return jax.shard_map(layer, mesh=finer, in_specs=in_specs, out_specs=out_specs, check_vma=False)
```

```python
import jax
import jax.numpy as jnp
from jax import lax
from jax.experimental import pallas as pl
from jax.experimental.pallas import tpu as pltpu
from jax.sharding import Mesh
from jax.sharding import PartitionSpec as P


EXPERTS = 8
SLOTS = 3
EP = ("ep_0", "ep_1", "ep_2")
PLANE = ("ep_1", "ep_2")
PAD = 24
ROWS = 24
LIVE = 20
MAIN = 1792
TAIL = 256
CHUNK = 80

epsilon = 1e-06
F32 = jnp.float32
BF16 = jnp.bfloat16


def swap(value):
    return lax.ppermute(value, "tp", [(0, 1), (1, 0)])


def along_z(value, shift):
    size = lax.axis_size("ep_0")
    return lax.ppermute(value, "ep_0", [(i, (i + shift) % size) for i in range(size)])


def dot(a, b):
    return jnp.dot(a, b, preferred_element_type=F32)


def dot_t(a, b):
    return lax.dot_general(a, b, (((1,), (1,)), ((), ())), preferred_element_type=F32)


def silu(v):
    return v / (1.0 + jnp.exp(-v))


def divided(index, by):
    return {3: (index * 43) >> 7, 5: (index * 13) >> 6, 24: (index * 171) >> 12}[by]


def iota2(shape, dim):
    return lax.broadcasted_iota(jnp.int32, shape, dim)


def one_hot(mask):
    return mask.astype(F32).astype(BF16)


def tail_maps(size, group):
    shape = (size, size)
    row, col = iota2(shape, 0), iota2(shape, 1)
    chunk = divided(row, ROWS)
    place = row - ROWS * chunk
    unpack = (place < LIVE) & (place >> 2 == group) & (col == ROWS * chunk + LIVE + (place & 3))
    pack = (place >= LIVE) & (col == ROWS * chunk + 4 * group + place - LIVE)
    return one_hot(unpack), one_hot(pack)


def branch_kernel(hidden, core_ref, x_ref, *refs):
    weights, pieces, (out_ref, full_ref, up_ref, down_ref, own_ref, other_ref, acc_ref, sem) = (
        refs[:6], refs[6:-8], refs[-8:],
    )
    half = own_ref.shape[1]
    count = len(pieces) // 2
    units = weights[0].shape[0]
    lanes = up_ref.shape[0] // 4
    copies = []

    def fetch(source, into):
        copies.append(pltpu.make_async_copy(source, into, sem.at[len(copies)]))
        copies[-1].start()

    for k, place in enumerate((0, 2, None, 1, 3, None)):
        if place is not None:
            fetch(weights[k], up_ref.at[pl.ds(place * lanes, units)])
    for k, place in ((2, 0), (5, 1)):
        fetch(weights[k], down_ref.at[pl.ds(place * lanes, units)])
    for k, piece in enumerate(pieces):
        into = (own_ref, other_ref)[k // count]
        fetch(piece, into.at[pl.ds((k % count) * CHUNK, CHUNK)])
    core = core_ref[0]
    here = pl.multiple_of(core * half, half)
    there = pl.multiple_of((1 - core) * half, half)
    total = x_ref.shape[0]
    step = total // 2
    groups = LIVE // 4
    maps = [tail_maps(step, g) for g in range(groups)]
    lane = iota2((step, 128), 1)
    for start in range(0, total, step):
        band = pl.ds(start, step)
        tail = jnp.zeros((step, TAIL), F32)
        w = jnp.zeros((step, 128), F32)
        for g in range(groups):
            tail = tail + dot(maps[g][0], x_ref[band, g * TAIL : (g + 1) * TAIL])
            w = w + jnp.where(
                lane == g, dot(maps[g][0], x_ref[band, groups * TAIL : groups * TAIL + 128]), 0.0
            )
        w = jnp.sum(w, axis=1, keepdims=True)
        full_ref[:, :MAIN] = x_ref[band, :]
        full_ref[:, MAIN:] = tail.astype(BF16)
        if start == 0:
            for copy in copies[:6]:
                copy.wait()
            for k in range(2):
                down_ref[k * lanes + units : (k + 1) * lanes, :] = jnp.zeros(
                    (lanes - units, 2 * half), BF16
                )
        pre = dot_t(full_ref[...], up_ref[...])
        h = w * silu(pre[:, : 2 * lanes]) * pre[:, 2 * lanes :]
        h = jnp.where((iota2(h.shape, 1) & (lanes - 1)) < units, h, 0.0).astype(BF16)
        acc_ref[...] = dot(h, down_ref[...])
        if start == 0:
            for copy in copies[6:]:
                copy.wait()
        pre = dot_t(full_ref[:, pl.ds(here, half)], own_ref[...])
        pre = pre + dot_t(full_ref[:, pl.ds(there, half)], other_ref[...])
        logit = pre[:, hidden : hidden + 1]
        gate = pltpu.roll(pre, 2 * PAD, 1)
        up = pltpu.roll(pre, PAD, 1)
        unit = iota2(pre.shape, 1) % CHUNK
        live = (unit >= 2 * PAD) & (unit < 2 * PAD + hidden)
        scale = 0.5 / (1.0 + jnp.exp(-logit))
        live = live & (w > 0.0)
        hd = jnp.where(live, scale * silu(gate) * up, 0.0).astype(BF16)
        acc_ref[:, pl.ds(here, half)] += dot(hd, own_ref[...])
        acc_ref[:, pl.ds(there, half)] += dot(hd, other_ref[...])
        tail = acc_ref[:, MAIN:].astype(BF16)
        for g in range(groups):
            part = slice(g * TAIL, (g + 1) * TAIL)
            out_ref[band, part] = (acc_ref[:, part] + dot(maps[g][1], tail)).astype(BF16)
        out_ref[band, groups * TAIL :] = acc_ref[:, groups * TAIL : MAIN].astype(BF16)


def in_vmem(value):
    return pltpu.with_memory_space_constraint(value, pltpu.VMEM)


def experts_and_dense(core, x, own, other, pieces, pieces2, hidden):
    rows, half = x.shape[0], pieces[0].shape[1]
    width = 2 * half
    vmem = pl.BlockSpec(memory_space=pltpu.VMEM)
    hbm = pl.BlockSpec(memory_space=pl.ANY)
    units = len(pieces) * CHUNK
    return pl.pallas_call(
        lambda *refs: branch_kernel(hidden, *refs),
        name="branch",
        out_shape=pltpu.VMEM((rows, MAIN), BF16),
        in_specs=[pl.BlockSpec(memory_space=pltpu.SMEM), vmem] + [hbm] * (6 + 2 * len(pieces)),
        out_specs=vmem,
        scratch_shapes=[
            pltpu.VMEM((rows // 2, width), BF16),
            pltpu.VMEM((4 * 128, width), BF16),
            pltpu.VMEM((2 * 128, width), BF16),
            pltpu.VMEM((units, half), BF16),
            pltpu.VMEM((units, half), BF16),
            pltpu.VMEM((rows // 2, width), F32),
            pltpu.SemaphoreType.DMA((6 + 2 * len(pieces),)),
        ],
    )(core.reshape(1), in_vmem(x), *own, *other, *pieces, *pieces2)


def slot_source(core, row):
    pair = divided(row, 5)
    place = row - 5 * pair
    crossed = place + jnp.where(place < SLOTS, SLOTS, -SLOTS)
    return 6 * pair + jnp.where(core == 0, place, crossed)


def spread_kernel(core_ref, x_ref, out_ref, rows_ref):
    core = core_ref[0]
    for k in range(x_ref.shape[0]):
        rows_ref[k * SLOTS : (k + 1) * SLOTS, :] = x_ref[k].astype(F32)
    x = rows_ref[...].astype(BF16)
    width = MAIN + TAIL
    shape = (ROWS, ROWS)
    row, col = iota2(shape, 0), iota2(shape, 1)
    main = dot(one_hot((row < LIVE) & (col == slot_source(core, row))), x[:, :MAIN])
    groups = LIVE // 4
    lane = iota2((ROWS, 128), 1)
    weight = jnp.zeros((ROWS, 128), F32)
    parts = []
    for g in range(groups):
        pick = one_hot((row >= LIVE) & (col == slot_source(core, 4 * g + row - LIVE)))
        parts.append(main[:, g * TAIL : (g + 1) * TAIL] + dot(pick, x[:, MAIN:width]))
        weight = weight + jnp.where(lane == g, dot(pick, x[:, width:]), 0.0)
    parts.append(main[:, groups * TAIL : groups * TAIL + 128] + weight)
    parts.append(main[:, groups * TAIL + 128 :])
    packed = jnp.concatenate(parts, axis=1).astype(BF16)
    for k in range(out_ref.shape[0]):
        out_ref[k] = packed


def spread(core, x, chips):
    vmem = pl.BlockSpec(memory_space=pltpu.VMEM)
    return pl.pallas_call(
        spread_kernel,
        name="spread",
        out_shape=pltpu.VMEM((chips, ROWS, MAIN), BF16),
        in_specs=[pl.BlockSpec(memory_space=pltpu.SMEM), vmem],
        out_specs=vmem,
        scratch_shapes=[pltpu.VMEM((EXPERTS * SLOTS, x.shape[2]), F32)],
    )(core.reshape(1), in_vmem(x))


def collect_kernel(core_ref, x_ref, out_ref, rows_ref):
    core = core_ref[0]
    half = out_ref.shape[2]
    total = x_ref[0].astype(F32)
    for k in range(1, x_ref.shape[0]):
        total = total + x_ref[k].astype(F32)
    total = total.astype(BF16)
    shape = (ROWS, ROWS)
    row, col = iota2(shape, 0), iota2(shape, 1)
    rows_ref[:, :MAIN] = dot(one_hot((col < LIVE) & (row == slot_source(core, col))), total)
    tail = jnp.zeros((ROWS, TAIL), F32)
    for g in range(LIVE // 4):
        pick = one_hot((col >= LIVE) & (row == slot_source(core, 4 * g + col - LIVE)))
        tail = tail + dot(pick, total[:, g * TAIL : (g + 1) * TAIL])
    rows_ref[:, MAIN:] = tail
    for k in range(out_ref.shape[0]):
        at = k // 2 * SLOTS
        part = rows_ref[at : at + SLOTS, k % 2 * half : (k % 2 + 1) * half]
        out_ref[k] = part.astype(BF16)


def collect(core, x):
    vmem = pl.BlockSpec(memory_space=pltpu.VMEM)
    half = (MAIN + TAIL) // 2
    return pl.pallas_call(
        collect_kernel,
        name="collect",
        out_shape=pltpu.VMEM((2 * EXPERTS, SLOTS, half), BF16),
        in_specs=[pl.BlockSpec(memory_space=pltpu.SMEM), vmem],
        out_specs=vmem,
        scratch_shapes=[pltpu.VMEM((ROWS, MAIN + TAIL), F32)],
    )(core.reshape(1), in_vmem(x))


def mixer_kernel(
    core_ref, x_ref, y_ref, gain_ref, wq, wk, wv, wo, state_ref, mix_ref, new_hbm,
    new_ref, turn_ref, read_ref, sem,
):
    rows, half = x_ref.shape
    heads, head = state_ref.shape[1], state_ref.shape[2]
    core = core_ref[0]
    here = pl.multiple_of(core * half, half)
    there = pl.multiple_of((1 - core) * half, half)
    x = x_ref[...].astype(F32)
    y = y_ref[...].astype(F32)
    total = jnp.sum(x * x, axis=1, keepdims=True) + jnp.sum(y * y, axis=1, keepdims=True)
    scale = lax.rsqrt(total / (2 * half) + epsilon)
    x = (x * scale * gain_ref[:, pl.ds(here, half)]).astype(BF16)
    y = (y * scale * gain_ref[:, pl.ds(there, half)]).astype(BF16)

    def project(ref):
        both = dot(x, ref[pl.ds(here, half), :]) + dot(y, ref[pl.ds(there, half), :])
        return both.astype(BF16).astype(F32)

    query = project(wq)
    key = project(wk) * head ** (-0.5)
    value = project(wv)
    turn_ref[0] = query.T
    turn_ref[1] = key.T
    decays = [
        jnp.where(core == 0, 1.0 - 2.0 ** (-3 - 2 * h), 1.0 - 2.0 ** (-3 - 2 * (h + heads)))
        for h in range(heads)
    ]
    group = 4
    copies = []
    for s in range(rows):
        for h in range(heads):
            part = slice(h * head, (h + 1) * head)
            q = turn_ref[0, part, s : s + 1]
            k = turn_ref[1, part, s : s + 1]
            new = decays[h] * state_ref[s, h] + k * value[s : s + 1, part]
            new_ref[s, h] = new
            read_ref[s : s + 1, part] = jnp.sum(q * new, axis=0, keepdims=True)
        if s % group == group - 1:
            band = pl.ds(s + 1 - group, group)
            copy = pltpu.make_async_copy(new_ref.at[band], new_hbm.at[band], sem.at[s // group])
            copy.start()
            copies.append(copy)
    outs = []
    for h in range(heads):
        read = read_ref[:, h * head : (h + 1) * head]
        centre = jnp.mean(read, axis=1, keepdims=True)
        spread = jnp.mean(jnp.square(read - centre), axis=1, keepdims=True)
        outs.append(((read - centre) * lax.rsqrt(spread + epsilon)).astype(BF16))
    mix = jnp.zeros(mix_ref.shape, F32)
    for h in range(heads):
        mix = mix + dot(outs[h], wo[h * head : (h + 1) * head, :])
    mix_ref[...] = mix.astype(BF16)
    for copy in copies:
        copy.wait()


def mixer(core, own, other, gain, wq, wk, wv, wo, state):
    rows, half = own.shape
    heads, head = state.shape[1], state.shape[2]
    vmem = pl.BlockSpec(memory_space=pltpu.VMEM)
    return pl.pallas_call(
        mixer_kernel,
        name="mixer",
        out_shape=(
            pltpu.VMEM((rows, 2 * half), BF16),
            jax.ShapeDtypeStruct(state.shape, F32),
        ),
        in_specs=[pl.BlockSpec(memory_space=pltpu.SMEM)] + [vmem] * 8,
        out_specs=(vmem, pl.BlockSpec(memory_space=pl.ANY)),
        scratch_shapes=[
            pltpu.VMEM(state.shape, F32),
            pltpu.VMEM((2, heads * head, rows), F32),
            pltpu.VMEM((rows, heads * head), F32),
            pltpu.SemaphoreType.DMA((rows // 4,)),
        ],
    )(
        core.reshape(1), in_vmem(own), in_vmem(other), gain.reshape(1, 2 * half),
        wq, wk, wv, wo, state,
    )


def first_slot(odd, core):
    return jnp.where(odd == core, 0, SLOTS)


def slots_kernel(
    core_ref, x_ref, y_ref, mix_ref, mix2_ref, gain_ref, gain2_ref, routes_ref, weights_ref,
    slot_ref, after_ref,
):
    rows, half = x_ref.shape
    core, odd = core_ref[0], core_ref[1]
    here = pl.multiple_of(core * half, half)
    there = pl.multiple_of((1 - core) * half, half)

    def add(ref, at):
        total = mix_ref[:, pl.ds(at, half)].astype(F32) + mix2_ref[:, pl.ds(at, half)].astype(F32)
        return (ref[...].astype(F32) + total).astype(BF16)

    after = add(x_ref, here)
    after_ref[...] = after
    x = after.astype(F32)
    y = add(y_ref, there).astype(F32)
    total = jnp.sum(x * x, axis=1, keepdims=True) + jnp.sum(y * y, axis=1, keepdims=True)
    scale = lax.rsqrt(total / (2 * half) + epsilon)
    x = (x * scale * gain_ref[...]).astype(BF16)
    y = (y * scale * gain2_ref[...]).astype(BF16)

    shape = (EXPERTS * SLOTS, rows)
    slot = iota2(shape, 0)
    expert = divided(slot, 3)
    slot = slot - SLOTS * expert + first_slot(odd, core)
    first = (routes_ref[0:1, :] == expert).astype(F32)
    second = (routes_ref[1:2, :] == expert).astype(F32)
    member = first + second
    earlier = iota2((rows, rows), 0) < iota2((rows, rows), 1)
    place = dot(member.astype(BF16), one_hot(earlier))
    select = jnp.where(place == slot.astype(F32), member, 0.0)
    weight = first * weights_ref[0:1, :].astype(F32) + second * weights_ref[1:2, :].astype(F32)
    weight = jnp.sum(select * weight, axis=1, keepdims=True)
    weight = jnp.broadcast_to(weight, (EXPERTS * SLOTS, 128))
    select = select.astype(BF16)
    x, y = dot(select, x), dot(select, y)
    for k in range(EXPERTS):
        part = slice(k * SLOTS, (k + 1) * SLOTS)
        slot_ref[k, :, pl.ds(here, half)] = x[part].astype(BF16)
        slot_ref[k, :, pl.ds(there, half)] = y[part].astype(BF16)
        slot_ref[k, :, 2 * half :] = weight[part].astype(BF16)


def to_slots(place, own, other, mix, mix2, gain, gain2, routes, route_w):
    rows, half = own.shape
    vmem = pl.BlockSpec(memory_space=pltpu.VMEM)
    return pl.pallas_call(
        slots_kernel,
        name="slots",
        out_shape=(
            pltpu.VMEM((EXPERTS, SLOTS, 2 * half + 128), BF16),
            pltpu.VMEM((rows, half), BF16),
        ),
        in_specs=[pl.BlockSpec(memory_space=pltpu.SMEM)] + [vmem] * 8,
        out_specs=(vmem, vmem),
    )(
        place, in_vmem(own), in_vmem(other), in_vmem(mix), in_vmem(mix2),
        gain.reshape(1, half), in_vmem(gain2.reshape(1, half)), routes.T, route_w.T,
    )


def home_kernel(core_ref, home_ref, after_ref, routes_ref, out_ref, rows_ref):
    odd = core_ref[1]
    rows = after_ref.shape[0]
    count = home_ref.shape[0]
    for k in range(count):
        rows_ref[k * SLOTS : (k + 1) * SLOTS, :] = home_ref[k].astype(F32)
    shape = (rows, count * SLOTS)
    slot = iota2(shape, 1)
    source = divided(slot, 3)
    expert = source >> 1
    slot = slot - SLOTS * source + first_slot(odd, source & 1)
    member = (routes_ref[:, 0:1] == expert).astype(F32) + (routes_ref[:, 1:2] == expert).astype(F32)
    earlier = iota2((rows, rows), 1) < iota2((rows, rows), 0)
    place = dot(one_hot(earlier), member.astype(BF16))
    select = jnp.where(place == slot.astype(F32), member, 0.0).astype(BF16)
    total = after_ref[...].astype(F32) + dot(select, rows_ref[...].astype(BF16))
    out_ref[...] = total.astype(BF16)


def at_home(place, home, after, routes):
    vmem = pl.BlockSpec(memory_space=pltpu.VMEM)
    return pl.pallas_call(
        home_kernel,
        name="home",
        out_shape=jax.ShapeDtypeStruct(after.shape, BF16),
        in_specs=[pl.BlockSpec(memory_space=pltpu.SMEM)] + [vmem] * 3,
        out_specs=vmem,
        scratch_shapes=[pltpu.VMEM((home.shape[0] * SLOTS, home.shape[2]), F32)],
    )(place, in_vmem(home), in_vmem(after), routes)


def layer(
    tokens, state, norm_mix, w_query, w_key, w_value, w_out, norm_ffn, gate_vector,
    dense_gate, dense_up, dense_down, exp_gate, exp_up, exp_down, routes, route_w,
):
    core = lax.axis_index("tp")
    half = tokens.shape[1]
    hidden = dense_gate.shape[1]

    def fill(size):
        return jnp.zeros((size, half), BF16)

    other_x = swap(tokens)
    other_gain = swap(norm_ffn)
    packed = jnp.concatenate(
        [
            dense_gate.T,
            gate_vector[None],
            fill(PAD - hidden - 1),
            dense_up.T,
            fill(PAD - hidden),
            dense_down,
            fill(CHUNK - 2 * PAD - hidden),
        ],
        axis=0,
    )
    mine = (exp_gate[0].T, exp_up[0].T, exp_down[0])
    theirs = tuple(swap(weights) for weights in mine)

    mix, new_state = mixer(core, tokens, other_x, norm_mix, w_query, w_key, w_value, w_out, state)
    mix2 = swap(mix)
    place = jnp.stack([core, lax.axis_index("ep_0") % 2])
    slot_rows, after = to_slots(
        place, tokens, other_x, mix, mix2, norm_ffn, other_gain, routes, route_w
    )
    at_plane = lax.all_to_all(slot_rows, "ep_0", 0, 0, tiled=True)
    pieces = [packed]
    for shift in (4, 3, 5, 2, 6, 1, 7):
        pieces.append(along_z(packed, shift))
    pieces2 = [swap(piece) for piece in pieces]
    chips = lax.axis_size(PLANE)
    copies = spread(core, at_plane, chips)
    gathered = lax.all_to_all(copies, PLANE, 0, 0, tiled=True)
    partial = experts_and_dense(
        core, gathered.reshape(chips * ROWS, MAIN), mine, theirs, pieces, pieces2, hidden
    )
    back = lax.all_to_all(partial.reshape(chips, ROWS, MAIN), PLANE, 0, 0, tiled=True)
    send = collect(core, back)
    home = lax.all_to_all(send, ("ep_0", "tp"), 0, 0, tiled=True)
    return (at_home(place, home, after, routes), new_state)


def solution(mesh):
    finer = Mesh(mesh.devices.reshape(8, 4, 4, mesh.shape["tp"]), ("ep_0", "ep_1", "ep_2", "tp"))
    in_specs = (
        P(EP, "tp"),
        P(EP, "tp", None, None),
        P(),
        P(None, "tp"),
        P(None, "tp"),
        P(None, "tp"),
        P("tp", None),
        P("tp"),
        P("tp"),
        P("tp", EP),
        P("tp", EP),
        P(EP, "tp"),
        P(EP, None, "tp"),
        P(EP, None, "tp"),
        P(EP, "tp", None),
        P(EP, None),
        P(EP, None),
    )
    out_specs = (P(EP, "tp"), P(EP, "tp", None, None))
    return jax.shard_map(layer, mesh=finer, in_specs=in_specs, out_specs=out_specs, check_vma=False)
```

```python
import jax
import jax.numpy as jnp
from jax import lax
from jax.experimental import pallas as pl
from jax.experimental.pallas import tpu as pltpu
from jax.sharding import Mesh
from jax.sharding import PartitionSpec as P


EXPERTS = 8
SLOTS = 3
EP = ("ep_0", "ep_1", "ep_2")
PLANE = ("ep_1", "ep_2")
PAD = 24
ROWS = 24
LIVE = 20
MAIN = 1792
TAIL = 256
SENT = 72
CHUNK = 80

epsilon = 1e-06
F32 = jnp.float32
BF16 = jnp.bfloat16


def swap(value):
    return lax.ppermute(value, "tp", [(0, 1), (1, 0)])


def along_z(value, shift):
    size = lax.axis_size("ep_0")
    return lax.ppermute(value, "ep_0", [(i, (i + shift) % size) for i in range(size)])


def dot(a, b):
    return jnp.dot(a, b, preferred_element_type=F32)


def dot_t(a, b):
    return lax.dot_general(a, b, (((1,), (1,)), ((), ())), preferred_element_type=F32)


def silu(v):
    return v / (1.0 + jnp.exp(-v))


def divided(index, by):
    return {3: (index * 43) >> 7, 5: (index * 13) >> 6, 24: (index * 171) >> 12}[by]


def iota2(shape, dim):
    return lax.broadcasted_iota(jnp.int32, shape, dim)


def one_hot(mask):
    return mask.astype(F32).astype(BF16)


def tail_maps(size, group):
    shape = (size, size)
    row, col = iota2(shape, 0), iota2(shape, 1)
    chunk = divided(row, ROWS)
    place = row - ROWS * chunk
    unpack = (place < LIVE) & (place >> 2 == group) & (col == ROWS * chunk + LIVE + (place & 3))
    pack = (place >= LIVE) & (col == ROWS * chunk + 4 * group + place - LIVE)
    return one_hot(unpack), one_hot(pack)


def branch_kernel(hidden, core_ref, x_ref, *refs):
    weights, pieces, (out_ref, full_ref, up_ref, down_ref, own_ref, other_ref, acc_ref, sem) = (
        refs[:6], refs[6:-8], refs[-8:],
    )
    half = own_ref.shape[1]
    count = len(pieces) // 2
    units = weights[0].shape[0]
    lanes = up_ref.shape[0] // 4
    copies = []

    def fetch(source, into):
        copies.append(pltpu.make_async_copy(source, into, sem.at[len(copies)]))
        copies[-1].start()

    for k, place in enumerate((0, 2, None, 1, 3, None)):
        if place is not None:
            fetch(weights[k], up_ref.at[pl.ds(place * lanes, units)])
    for k, place in ((2, 0), (5, 1)):
        fetch(weights[k], down_ref.at[pl.ds(place * lanes, units)])
    for k, piece in enumerate(pieces):
        into = (own_ref, other_ref)[k // count]
        fetch(piece, into.at[pl.ds((k % count) * CHUNK, SENT)])
    core = core_ref[0]
    here = pl.multiple_of(core * half, half)
    there = pl.multiple_of((1 - core) * half, half)
    total = x_ref.shape[0]
    step = total // 2
    bands = [pl.ds(start, step) for start in range(0, total, step)]
    groups = LIVE // 4
    maps = [tail_maps(step, g) for g in range(groups)]
    lane = iota2((step, 128), 1)
    weight = []
    for band in bands:
        tail = jnp.zeros((step, TAIL), F32)
        w = jnp.zeros((step, 128), F32)
        for g in range(groups):
            tail = tail + dot(maps[g][0], x_ref[band, g * TAIL : (g + 1) * TAIL])
            w = w + jnp.where(
                lane == g, dot(maps[g][0], x_ref[band, groups * TAIL : groups * TAIL + 128]), 0.0
            )
        weight.append(jnp.sum(w, axis=1, keepdims=True))
        full_ref[band, :MAIN] = x_ref[band, :]
        full_ref[band, MAIN:] = tail.astype(BF16)
    w = jnp.concatenate(weight, axis=0)
    for copy in copies[:6]:
        copy.wait()
    for k in range(2):
        down_ref[k * lanes + units : (k + 1) * lanes, :] = jnp.zeros(
            (lanes - units, 2 * half), BF16
        )
    pre = dot_t(full_ref[...], up_ref[...])
    h = w * silu(pre[:, : 2 * lanes]) * pre[:, 2 * lanes :]
    h = jnp.where((iota2(h.shape, 1) & (lanes - 1)) < units, h, 0.0).astype(BF16)
    acc_ref[...] = dot(h, down_ref[...])
    for copy in copies[6:]:
        copy.wait()
    for ref in (own_ref, other_ref):
        for k in range(count):
            ref[k * CHUNK + SENT : (k + 1) * CHUNK, :] = jnp.zeros((CHUNK - SENT, half), BF16)
    pre = dot_t(full_ref[:, pl.ds(here, half)], own_ref[...])
    pre = pre + dot_t(full_ref[:, pl.ds(there, half)], other_ref[...])
    logit = pre[:, hidden : hidden + 1]
    gate = pltpu.roll(pre, 2 * PAD, 1)
    up = pltpu.roll(pre, PAD, 1)
    unit = iota2(pre.shape, 1) % CHUNK
    live = (unit >= 2 * PAD) & (unit < 2 * PAD + hidden) & (w > 0.0)
    scale = 0.5 / (1.0 + jnp.exp(-logit))
    hd = jnp.where(live, scale * silu(gate) * up, 0.0).astype(BF16)
    acc_ref[:, pl.ds(here, half)] += dot(hd, own_ref[...])
    acc_ref[:, pl.ds(there, half)] += dot(hd, other_ref[...])
    for band in bands:
        tail = acc_ref[band, MAIN:].astype(BF16)
        for g in range(groups):
            part = slice(g * TAIL, (g + 1) * TAIL)
            out_ref[band, part] = (acc_ref[band, part] + dot(maps[g][1], tail)).astype(BF16)
        out_ref[band, groups * TAIL :] = acc_ref[band, groups * TAIL : MAIN].astype(BF16)


def in_vmem(value):
    return pltpu.with_memory_space_constraint(value, pltpu.VMEM)


def experts_and_dense(core, x, own, other, pieces, pieces2, hidden):
    rows, half = x.shape[0], pieces[0].shape[1]
    width = 2 * half
    vmem = pl.BlockSpec(memory_space=pltpu.VMEM)
    hbm = pl.BlockSpec(memory_space=pl.ANY)
    units = len(pieces) * CHUNK
    return pl.pallas_call(
        lambda *refs: branch_kernel(hidden, *refs),
        name="branch",
        out_shape=pltpu.VMEM((rows, MAIN), BF16),
        in_specs=[pl.BlockSpec(memory_space=pltpu.SMEM), vmem] + [hbm] * (6 + 2 * len(pieces)),
        out_specs=vmem,
        scratch_shapes=[
            pltpu.VMEM((rows, width), BF16),
            pltpu.VMEM((4 * 128, width), BF16),
            pltpu.VMEM((2 * 128, width), BF16),
            pltpu.VMEM((units, half), BF16),
            pltpu.VMEM((units, half), BF16),
            pltpu.VMEM((rows, width), F32),
            pltpu.SemaphoreType.DMA((6 + 2 * len(pieces),)),
        ],
    )(core.reshape(1), in_vmem(x), *own, *other, *pieces, *pieces2)


def slot_source(core, row):
    pair = divided(row, 5)
    place = row - 5 * pair
    crossed = place + jnp.where(place < SLOTS, SLOTS, -SLOTS)
    return 6 * pair + jnp.where(core == 0, place, crossed)


def spread_kernel(core_ref, x_ref, out_ref, rows_ref):
    core = core_ref[0]
    for k in range(x_ref.shape[0]):
        rows_ref[k * SLOTS : (k + 1) * SLOTS, :] = x_ref[k].astype(F32)
    x = rows_ref[...].astype(BF16)
    width = MAIN + TAIL
    shape = (ROWS, ROWS)
    row, col = iota2(shape, 0), iota2(shape, 1)
    main = dot(one_hot((row < LIVE) & (col == slot_source(core, row))), x[:, :MAIN])
    groups = LIVE // 4
    lane = iota2((ROWS, 128), 1)
    weight = jnp.zeros((ROWS, 128), F32)
    parts = []
    for g in range(groups):
        pick = one_hot((row >= LIVE) & (col == slot_source(core, 4 * g + row - LIVE)))
        parts.append(main[:, g * TAIL : (g + 1) * TAIL] + dot(pick, x[:, MAIN:width]))
        weight = weight + jnp.where(lane == g, dot(pick, x[:, width:]), 0.0)
    parts.append(main[:, groups * TAIL : groups * TAIL + 128] + weight)
    parts.append(main[:, groups * TAIL + 128 :])
    packed = jnp.concatenate(parts, axis=1).astype(BF16)
    for k in range(out_ref.shape[0]):
        out_ref[k] = packed


def spread(core, x, chips):
    vmem = pl.BlockSpec(memory_space=pltpu.VMEM)
    return pl.pallas_call(
        spread_kernel,
        name="spread",
        out_shape=pltpu.VMEM((chips, ROWS, MAIN), BF16),
        in_specs=[pl.BlockSpec(memory_space=pltpu.SMEM), vmem],
        out_specs=vmem,
        scratch_shapes=[pltpu.VMEM((EXPERTS * SLOTS, x.shape[2]), F32)],
    )(core.reshape(1), in_vmem(x))


def collect_kernel(core_ref, x_ref, out_ref, rows_ref):
    core = core_ref[0]
    half = out_ref.shape[2]
    total = x_ref[0].astype(F32)
    for k in range(1, x_ref.shape[0]):
        total = total + x_ref[k].astype(F32)
    total = total.astype(BF16)
    shape = (ROWS, ROWS)
    row, col = iota2(shape, 0), iota2(shape, 1)
    rows_ref[:, :MAIN] = dot(one_hot((col < LIVE) & (row == slot_source(core, col))), total)
    tail = jnp.zeros((ROWS, TAIL), F32)
    for g in range(LIVE // 4):
        pick = one_hot((col >= LIVE) & (row == slot_source(core, 4 * g + col - LIVE)))
        tail = tail + dot(pick, total[:, g * TAIL : (g + 1) * TAIL])
    rows_ref[:, MAIN:] = tail
    for k in range(out_ref.shape[0]):
        at = k // 2 * SLOTS
        part = rows_ref[at : at + SLOTS, k % 2 * half : (k % 2 + 1) * half]
        out_ref[k] = part.astype(BF16)


def collect(core, x):
    vmem = pl.BlockSpec(memory_space=pltpu.VMEM)
    half = (MAIN + TAIL) // 2
    return pl.pallas_call(
        collect_kernel,
        name="collect",
        out_shape=pltpu.VMEM((2 * EXPERTS, SLOTS, half), BF16),
        in_specs=[pl.BlockSpec(memory_space=pltpu.SMEM), vmem],
        out_specs=vmem,
        scratch_shapes=[pltpu.VMEM((ROWS, MAIN + TAIL), F32)],
    )(core.reshape(1), in_vmem(x))


def mixer_kernel(
    core_ref, x_ref, y_ref, gain_ref, wq_hbm, wk_hbm, wv_hbm, wo_hbm, state_hbm, mix_ref, new_hbm,
    wq, wk, wv, wo, state_ref, new_ref, turn_ref, read_ref, sem, load_sem,
):
    rows, half = x_ref.shape
    heads, head = state_ref.shape[1], state_ref.shape[2]
    loads = []
    pairs = ((wq_hbm, wq), (wk_hbm, wk), (wv_hbm, wv), (state_hbm, state_ref), (wo_hbm, wo))
    for k, (source, into) in enumerate(pairs):
        loads.append(pltpu.make_async_copy(source, into, load_sem.at[k]))
        loads[-1].start()
    core = core_ref[0]
    here = pl.multiple_of(core * half, half)
    there = pl.multiple_of((1 - core) * half, half)
    x = x_ref[...].astype(F32)
    y = y_ref[...].astype(F32)
    total = jnp.sum(x * x, axis=1, keepdims=True) + jnp.sum(y * y, axis=1, keepdims=True)
    scale = lax.rsqrt(total / (2 * half) + epsilon)
    x = (x * scale * gain_ref[:, pl.ds(here, half)]).astype(BF16)
    y = (y * scale * gain_ref[:, pl.ds(there, half)]).astype(BF16)

    def project(ref):
        both = dot(x, ref[pl.ds(here, half), :]) + dot(y, ref[pl.ds(there, half), :])
        return both.astype(BF16).astype(F32)

    loads[0].wait()
    query = project(wq)
    loads[1].wait()
    key = project(wk) * head ** (-0.5)
    loads[2].wait()
    value = project(wv)
    turn_ref[0] = query.T
    turn_ref[1] = key.T
    decays = [
        jnp.where(core == 0, 1.0 - 2.0 ** (-3 - 2 * h), 1.0 - 2.0 ** (-3 - 2 * (h + heads)))
        for h in range(heads)
    ]
    loads[3].wait()
    group = 4
    copies = []
    for s in range(rows):
        for h in range(heads):
            part = slice(h * head, (h + 1) * head)
            q = turn_ref[0, part, s : s + 1]
            k = turn_ref[1, part, s : s + 1]
            new = decays[h] * state_ref[s, h] + k * value[s : s + 1, part]
            new_ref[s, h] = new
            read_ref[s : s + 1, part] = jnp.sum(q * new, axis=0, keepdims=True)
        if s % group == group - 1:
            band = pl.ds(s + 1 - group, group)
            copy = pltpu.make_async_copy(new_ref.at[band], new_hbm.at[band], sem.at[s // group])
            copy.start()
            copies.append(copy)
    outs = []
    for h in range(heads):
        read = read_ref[:, h * head : (h + 1) * head]
        centre = jnp.mean(read, axis=1, keepdims=True)
        spread = jnp.mean(jnp.square(read - centre), axis=1, keepdims=True)
        outs.append(((read - centre) * lax.rsqrt(spread + epsilon)).astype(BF16))
    loads[4].wait()
    mix = jnp.zeros(mix_ref.shape, F32)
    for h in range(heads):
        mix = mix + dot(outs[h], wo[h * head : (h + 1) * head, :])
    mix_ref[...] = mix.astype(BF16)
    for copy in copies:
        copy.wait()


def mixer(core, own, other, gain, wq, wk, wv, wo, state):
    rows, half = own.shape
    heads, head = state.shape[1], state.shape[2]
    vmem = pl.BlockSpec(memory_space=pltpu.VMEM)
    hbm = pl.BlockSpec(memory_space=pl.ANY)
    return pl.pallas_call(
        mixer_kernel,
        name="mixer",
        out_shape=(
            pltpu.VMEM((rows, 2 * half), BF16),
            jax.ShapeDtypeStruct(state.shape, F32),
        ),
        in_specs=[pl.BlockSpec(memory_space=pltpu.SMEM)] + [vmem] * 3 + [hbm] * 5,
        out_specs=(vmem, hbm),
        scratch_shapes=[
            pltpu.VMEM(wq.shape, BF16),
            pltpu.VMEM(wk.shape, BF16),
            pltpu.VMEM(wv.shape, BF16),
            pltpu.VMEM(wo.shape, BF16),
            pltpu.VMEM(state.shape, F32),
            pltpu.VMEM(state.shape, F32),
            pltpu.VMEM((2, heads * head, rows), F32),
            pltpu.VMEM((rows, heads * head), F32),
            pltpu.SemaphoreType.DMA((rows // 4,)),
            pltpu.SemaphoreType.DMA((5,)),
        ],
    )(
        core.reshape(1), in_vmem(own), in_vmem(other), gain.reshape(1, 2 * half),
        wq, wk, wv, wo, state,
    )


def first_slot(odd, core):
    return jnp.where(odd == core, 0, SLOTS)


def slots_kernel(
    core_ref, x_ref, y_ref, mix_ref, mix2_ref, gain_ref, gain2_ref, routes_ref, weights_ref,
    slot_ref, after_ref,
):
    rows, half = x_ref.shape
    core, odd = core_ref[0], core_ref[1]
    here = pl.multiple_of(core * half, half)
    there = pl.multiple_of((1 - core) * half, half)

    def add(ref, at):
        total = mix_ref[:, pl.ds(at, half)].astype(F32) + mix2_ref[:, pl.ds(at, half)].astype(F32)
        return (ref[...].astype(F32) + total).astype(BF16)

    after = add(x_ref, here)
    after_ref[...] = after
    x = after.astype(F32)
    y = add(y_ref, there).astype(F32)
    total = jnp.sum(x * x, axis=1, keepdims=True) + jnp.sum(y * y, axis=1, keepdims=True)
    scale = lax.rsqrt(total / (2 * half) + epsilon)
    x = (x * scale * gain_ref[...]).astype(BF16)
    y = (y * scale * gain2_ref[...]).astype(BF16)

    shape = (EXPERTS * SLOTS, rows)
    slot = iota2(shape, 0)
    expert = divided(slot, 3)
    slot = slot - SLOTS * expert + first_slot(odd, core)
    first = (routes_ref[0:1, :] == expert).astype(F32)
    second = (routes_ref[1:2, :] == expert).astype(F32)
    member = first + second
    earlier = iota2((rows, rows), 0) < iota2((rows, rows), 1)
    place = dot(member.astype(BF16), one_hot(earlier))
    select = jnp.where(place == slot.astype(F32), member, 0.0)
    weight = first * weights_ref[0:1, :].astype(F32) + second * weights_ref[1:2, :].astype(F32)
    weight = jnp.sum(select * weight, axis=1, keepdims=True)
    weight = jnp.broadcast_to(weight, (EXPERTS * SLOTS, 128))
    select = select.astype(BF16)
    x, y = dot(select, x), dot(select, y)
    for k in range(EXPERTS):
        part = slice(k * SLOTS, (k + 1) * SLOTS)
        slot_ref[k, :, pl.ds(here, half)] = x[part].astype(BF16)
        slot_ref[k, :, pl.ds(there, half)] = y[part].astype(BF16)
        slot_ref[k, :, 2 * half :] = weight[part].astype(BF16)


def to_slots(place, own, other, mix, mix2, gain, gain2, routes, route_w):
    rows, half = own.shape
    vmem = pl.BlockSpec(memory_space=pltpu.VMEM)
    return pl.pallas_call(
        slots_kernel,
        name="slots",
        out_shape=(
            pltpu.VMEM((EXPERTS, SLOTS, 2 * half + 128), BF16),
            pltpu.VMEM((rows, half), BF16),
        ),
        in_specs=[pl.BlockSpec(memory_space=pltpu.SMEM)] + [vmem] * 8,
        out_specs=(vmem, vmem),
    )(
        place, in_vmem(own), in_vmem(other), in_vmem(mix), in_vmem(mix2),
        gain.reshape(1, half), in_vmem(gain2.reshape(1, half)), routes.T, route_w.T,
    )


def home_kernel(core_ref, home_ref, after_ref, routes_ref, out_ref, rows_ref):
    odd = core_ref[1]
    rows = after_ref.shape[0]
    count = home_ref.shape[0]
    for k in range(count):
        rows_ref[k * SLOTS : (k + 1) * SLOTS, :] = home_ref[k].astype(F32)
    shape = (rows, count * SLOTS)
    slot = iota2(shape, 1)
    source = divided(slot, 3)
    expert = source >> 1
    slot = slot - SLOTS * source + first_slot(odd, source & 1)
    member = (routes_ref[:, 0:1] == expert).astype(F32) + (routes_ref[:, 1:2] == expert).astype(F32)
    earlier = iota2((rows, rows), 1) < iota2((rows, rows), 0)
    place = dot(one_hot(earlier), member.astype(BF16))
    select = jnp.where(place == slot.astype(F32), member, 0.0).astype(BF16)
    total = after_ref[...].astype(F32) + dot(select, rows_ref[...].astype(BF16))
    out_ref[...] = total.astype(BF16)


def at_home(place, home, after, routes):
    vmem = pl.BlockSpec(memory_space=pltpu.VMEM)
    return pl.pallas_call(
        home_kernel,
        name="home",
        out_shape=jax.ShapeDtypeStruct(after.shape, BF16),
        in_specs=[pl.BlockSpec(memory_space=pltpu.SMEM)] + [vmem] * 3,
        out_specs=vmem,
        scratch_shapes=[pltpu.VMEM((home.shape[0] * SLOTS, home.shape[2]), F32)],
    )(place, in_vmem(home), in_vmem(after), routes)


def layer(
    tokens, state, norm_mix, w_query, w_key, w_value, w_out, norm_ffn, gate_vector,
    dense_gate, dense_up, dense_down, exp_gate, exp_up, exp_down, routes, route_w,
):
    core = lax.axis_index("tp")
    half = tokens.shape[1]
    hidden = dense_gate.shape[1]

    def fill(size):
        return jnp.zeros((size, half), BF16)

    other_x = swap(tokens)
    other_gain = swap(norm_ffn)
    packed = jnp.concatenate(
        [
            dense_gate.T,
            gate_vector[None],
            fill(PAD - hidden - 1),
            dense_up.T,
            fill(PAD - hidden),
            dense_down,
            fill(SENT - 2 * PAD - hidden),
        ],
        axis=0,
    )
    mine = (exp_gate[0].T, exp_up[0].T, exp_down[0])
    theirs = tuple(swap(weights) for weights in mine)

    mix, new_state = mixer(core, tokens, other_x, norm_mix, w_query, w_key, w_value, w_out, state)
    mix2 = swap(mix)
    place = jnp.stack([core, lax.axis_index("ep_0") % 2])
    slot_rows, after = to_slots(
        place, tokens, other_x, mix, mix2, norm_ffn, other_gain, routes, route_w
    )
    at_plane = lax.all_to_all(slot_rows, "ep_0", 0, 0, tiled=True)
    pieces = [packed]
    for shift in (4, 3, 5, 2, 6, 1, 7):
        pieces.append(along_z(packed, shift))
    pieces2 = [swap(piece) for piece in pieces]
    chips = lax.axis_size(PLANE)
    copies = spread(core, at_plane, chips)
    gathered = lax.all_to_all(copies, PLANE, 0, 0, tiled=True)
    partial = experts_and_dense(
        core, gathered.reshape(chips * ROWS, MAIN), mine, theirs, pieces, pieces2, hidden
    )
    back = lax.all_to_all(partial.reshape(chips, ROWS, MAIN), PLANE, 0, 0, tiled=True)
    send = collect(core, back)
    home = lax.all_to_all(send, ("ep_0", "tp"), 0, 0, tiled=True)
    return (at_home(place, home, after, routes), new_state)


def solution(mesh):
    finer = Mesh(mesh.devices.reshape(8, 4, 4, mesh.shape["tp"]), ("ep_0", "ep_1", "ep_2", "tp"))
    in_specs = (
        P(EP, "tp"),
        P(EP, "tp", None, None),
        P(),
        P(None, "tp"),
        P(None, "tp"),
        P(None, "tp"),
        P("tp", None),
        P("tp"),
        P("tp"),
        P("tp", EP),
        P("tp", EP),
        P(EP, "tp"),
        P(EP, None, "tp"),
        P(EP, None, "tp"),
        P(EP, "tp", None),
        P(EP, None),
        P(EP, None),
    )
    out_specs = (P(EP, "tp"), P(EP, "tp", None, None))
    return jax.shard_map(layer, mesh=finer, in_specs=in_specs, out_specs=out_specs, check_vma=False)
```

```python
import jax
import jax.numpy as jnp
from jax import lax
from jax.experimental import pallas as pl
from jax.experimental.pallas import tpu as pltpu
from jax.sharding import Mesh
from jax.sharding import PartitionSpec as P


EXPERTS = 8
SLOTS = 3
EP = ("ep_0", "ep_1", "ep_2")
PLANE = ("ep_1", "ep_2")
PAD = 24
ROWS = 24
LIVE = 20
MAIN = 1792
TAIL = 256
SENT = 72
CHUNK = 80

epsilon = 1e-06
F32 = jnp.float32
BF16 = jnp.bfloat16


def swap(value):
    return lax.ppermute(value, "tp", [(0, 1), (1, 0)])


def along_z(value, shift):
    size = lax.axis_size("ep_0")
    return lax.ppermute(value, "ep_0", [(i, (i + shift) % size) for i in range(size)])


def dot(a, b):
    return jnp.dot(a, b, preferred_element_type=F32)


def dot_t(a, b):
    return lax.dot_general(a, b, (((1,), (1,)), ((), ())), preferred_element_type=F32)


def silu(v):
    return v / (1.0 + jnp.exp(-v))


def divided(index, by):
    return {3: (index * 43) >> 7, 5: (index * 13) >> 6, 24: (index * 171) >> 12}[by]


def iota2(shape, dim):
    return lax.broadcasted_iota(jnp.int32, shape, dim)


def one_hot(mask):
    return mask.astype(F32).astype(BF16)


def tail_maps(size, group):
    shape = (size, size)
    row, col = iota2(shape, 0), iota2(shape, 1)
    chunk = divided(row, ROWS)
    place = row - ROWS * chunk
    unpack = (place < LIVE) & (place >> 2 == group) & (col == ROWS * chunk + LIVE + (place & 3))
    pack = (place >= LIVE) & (col == ROWS * chunk + 4 * group + place - LIVE)
    return one_hot(unpack), one_hot(pack)


def branch_kernel(hidden, core_ref, x_ref, *refs):
    weights, pieces, (out_ref, full_ref, up_ref, down_ref, own_ref, other_ref, acc_ref, sem) = (
        refs[:6], refs[6:-8], refs[-8:],
    )
    half = own_ref.shape[1]
    count = len(pieces) // 2
    units = weights[0].shape[0]
    lanes = up_ref.shape[0] // 4
    copies = []

    def fetch(source, into):
        copies.append(pltpu.make_async_copy(source, into, sem.at[len(copies)]))
        copies[-1].start()

    for k, place in enumerate((0, 2, None, 1, 3, None)):
        if place is not None:
            fetch(weights[k], up_ref.at[pl.ds(place * lanes, units)])
    for k, place in ((2, 0), (5, 1)):
        fetch(weights[k], down_ref.at[pl.ds(place * lanes, units)])
    for k, piece in enumerate(pieces):
        into = (own_ref, other_ref)[k // count]
        fetch(piece, into.at[pl.ds((k % count) * CHUNK, SENT)])
    core = core_ref[0]
    here = pl.multiple_of(core * half, half)
    there = pl.multiple_of((1 - core) * half, half)
    total = x_ref.shape[0]
    step = total // 2
    bands = [pl.ds(start, step) for start in range(0, total, step)]
    groups = LIVE // 4
    maps = [tail_maps(step, g) for g in range(groups)]
    lane = iota2((step, 128), 1)
    weight = []
    for band in bands:
        tail = jnp.zeros((step, TAIL), F32)
        w = jnp.zeros((step, 128), F32)
        for g in range(groups):
            tail = tail + dot(maps[g][0], x_ref[band, g * TAIL : (g + 1) * TAIL])
            w = w + jnp.where(
                lane == g, dot(maps[g][0], x_ref[band, groups * TAIL : groups * TAIL + 128]), 0.0
            )
        weight.append(jnp.sum(w, axis=1, keepdims=True))
        full_ref[band, :MAIN] = x_ref[band, :]
        full_ref[band, MAIN:] = tail.astype(BF16)
    w = jnp.concatenate(weight, axis=0)
    for copy in copies[:6]:
        copy.wait()
    for k in range(2):
        down_ref[k * lanes + units : (k + 1) * lanes, :] = jnp.zeros(
            (lanes - units, 2 * half), BF16
        )
    pre = dot_t(full_ref[...], up_ref[...])
    h = w * silu(pre[:, : 2 * lanes]) * pre[:, 2 * lanes :]
    h = jnp.where((iota2(h.shape, 1) & (lanes - 1)) < units, h, 0.0).astype(BF16)
    acc_ref[...] = dot(h, down_ref[...])
    for copy in copies[6:]:
        copy.wait()
    for ref in (own_ref, other_ref):
        for k in range(count):
            ref[k * CHUNK + SENT : (k + 1) * CHUNK, :] = jnp.zeros((CHUNK - SENT, half), BF16)
    pre = dot_t(full_ref[:, pl.ds(here, half)], own_ref[...])
    pre = pre + dot_t(full_ref[:, pl.ds(there, half)], other_ref[...])
    logit = pre[:, hidden : hidden + 1]
    gate = pltpu.roll(pre, 2 * PAD, 1)
    up = pltpu.roll(pre, PAD, 1)
    unit = iota2(pre.shape, 1) % CHUNK
    live = (unit >= 2 * PAD) & (unit < 2 * PAD + hidden) & (w > 0.0)
    scale = 0.5 / (1.0 + jnp.exp(-logit))
    hd = jnp.where(live, scale * silu(gate) * up, 0.0).astype(BF16)
    acc_ref[:, pl.ds(here, half)] += dot(hd, own_ref[...])
    acc_ref[:, pl.ds(there, half)] += dot(hd, other_ref[...])
    for band in bands:
        tail = acc_ref[band, MAIN:].astype(BF16)
        for g in range(groups):
            part = slice(g * TAIL, (g + 1) * TAIL)
            out_ref[band, part] = (acc_ref[band, part] + dot(maps[g][1], tail)).astype(BF16)
        out_ref[band, groups * TAIL :] = acc_ref[band, groups * TAIL : MAIN].astype(BF16)


def in_vmem(value):
    return pltpu.with_memory_space_constraint(value, pltpu.VMEM)


def experts_and_dense(core, x, own, other, pieces, pieces2, hidden):
    rows, half = x.shape[0], pieces[0].shape[1]
    width = 2 * half
    vmem = pl.BlockSpec(memory_space=pltpu.VMEM)
    hbm = pl.BlockSpec(memory_space=pl.ANY)
    units = len(pieces) * CHUNK
    return pl.pallas_call(
        lambda *refs: branch_kernel(hidden, *refs),
        name="branch",
        out_shape=pltpu.VMEM((rows, MAIN), BF16),
        in_specs=[pl.BlockSpec(memory_space=pltpu.SMEM), vmem] + [hbm] * (6 + 2 * len(pieces)),
        out_specs=vmem,
        scratch_shapes=[
            pltpu.VMEM((rows, width), BF16),
            pltpu.VMEM((4 * 128, width), BF16),
            pltpu.VMEM((2 * 128, width), BF16),
            pltpu.VMEM((units, half), BF16),
            pltpu.VMEM((units, half), BF16),
            pltpu.VMEM((rows, width), F32),
            pltpu.SemaphoreType.DMA((6 + 2 * len(pieces),)),
        ],
    )(core.reshape(1), in_vmem(x), *own, *other, *pieces, *pieces2)


def slot_source(core, row):
    pair = divided(row, 5)
    place = row - 5 * pair
    crossed = place + jnp.where(place < SLOTS, SLOTS, -SLOTS)
    return 6 * pair + jnp.where(core == 0, place, crossed)


def spread_kernel(core_ref, x_ref, out_ref, rows_ref):
    core = core_ref[0]
    for k in range(x_ref.shape[0]):
        rows_ref[k * SLOTS : (k + 1) * SLOTS, :] = x_ref[k].astype(F32)
    x = rows_ref[...].astype(BF16)
    width = MAIN + TAIL
    shape = (ROWS, ROWS)
    row, col = iota2(shape, 0), iota2(shape, 1)
    main = dot(one_hot((row < LIVE) & (col == slot_source(core, row))), x[:, :MAIN])
    groups = LIVE // 4
    lane = iota2((ROWS, 128), 1)
    weight = jnp.zeros((ROWS, 128), F32)
    parts = []
    for g in range(groups):
        pick = one_hot((row >= LIVE) & (col == slot_source(core, 4 * g + row - LIVE)))
        parts.append(main[:, g * TAIL : (g + 1) * TAIL] + dot(pick, x[:, MAIN:width]))
        weight = weight + jnp.where(lane == g, dot(pick, x[:, width:]), 0.0)
    parts.append(main[:, groups * TAIL : groups * TAIL + 128] + weight)
    parts.append(main[:, groups * TAIL + 128 :])
    packed = jnp.concatenate(parts, axis=1).astype(BF16)
    for k in range(out_ref.shape[0]):
        out_ref[k] = packed


def spread(core, x, chips):
    vmem = pl.BlockSpec(memory_space=pltpu.VMEM)
    return pl.pallas_call(
        spread_kernel,
        name="spread",
        out_shape=pltpu.VMEM((chips, ROWS, MAIN), BF16),
        in_specs=[pl.BlockSpec(memory_space=pltpu.SMEM), vmem],
        out_specs=vmem,
        scratch_shapes=[pltpu.VMEM((EXPERTS * SLOTS, x.shape[2]), F32)],
    )(core.reshape(1), in_vmem(x))


def collect_kernel(core_ref, x_ref, out_ref, rows_ref):
    core = core_ref[0]
    half = out_ref.shape[2]
    total = x_ref[0].astype(F32)
    for k in range(1, x_ref.shape[0]):
        total = total + x_ref[k].astype(F32)
    total = total.astype(BF16)
    shape = (ROWS, ROWS)
    row, col = iota2(shape, 0), iota2(shape, 1)
    rows_ref[:, :MAIN] = dot(one_hot((col < LIVE) & (row == slot_source(core, col))), total)
    tail = jnp.zeros((ROWS, TAIL), F32)
    for g in range(LIVE // 4):
        pick = one_hot((col >= LIVE) & (row == slot_source(core, 4 * g + col - LIVE)))
        tail = tail + dot(pick, total[:, g * TAIL : (g + 1) * TAIL])
    rows_ref[:, MAIN:] = tail
    for k in range(out_ref.shape[0]):
        at = k // 2 * SLOTS
        part = rows_ref[at : at + SLOTS, k % 2 * half : (k % 2 + 1) * half]
        out_ref[k] = part.astype(BF16)


def collect(core, x):
    vmem = pl.BlockSpec(memory_space=pltpu.VMEM)
    half = (MAIN + TAIL) // 2
    return pl.pallas_call(
        collect_kernel,
        name="collect",
        out_shape=pltpu.VMEM((2 * EXPERTS, SLOTS, half), BF16),
        in_specs=[pl.BlockSpec(memory_space=pltpu.SMEM), vmem],
        out_specs=vmem,
        scratch_shapes=[pltpu.VMEM((ROWS, MAIN + TAIL), F32)],
    )(core.reshape(1), in_vmem(x))


def mixer_kernel(
    core_ref, x_hbm, y_ref, gain_ref, wq_hbm, wk_hbm, wv_hbm, wo_hbm, state_hbm, mix_ref, new_hbm,
    x_ref, wq, wk, wv, wo, state_ref, new_ref, turn_ref, read_ref, sem, load_sem,
):
    rows, half = x_ref.shape
    heads, head = state_ref.shape[1], state_ref.shape[2]
    loads = []
    pairs = ((x_hbm, x_ref), (wq_hbm, wq), (wk_hbm, wk), (wv_hbm, wv), (state_hbm, state_ref), (wo_hbm, wo))
    for k, (source, into) in enumerate(pairs):
        loads.append(pltpu.make_async_copy(source, into, load_sem.at[k]))
        loads[-1].start()
    core = core_ref[0]
    here = pl.multiple_of(core * half, half)
    there = pl.multiple_of((1 - core) * half, half)
    loads[0].wait()
    x = x_ref[...].astype(F32)
    y = y_ref[...].astype(F32)
    total = jnp.sum(x * x, axis=1, keepdims=True) + jnp.sum(y * y, axis=1, keepdims=True)
    scale = lax.rsqrt(total / (2 * half) + epsilon)
    x = (x * scale * gain_ref[:, pl.ds(here, half)]).astype(BF16)
    y = (y * scale * gain_ref[:, pl.ds(there, half)]).astype(BF16)

    def project(ref):
        both = dot(x, ref[pl.ds(here, half), :]) + dot(y, ref[pl.ds(there, half), :])
        return both.astype(BF16).astype(F32)

    loads[1].wait()
    query = project(wq)
    loads[2].wait()
    key = project(wk) * head ** (-0.5)
    loads[3].wait()
    value = project(wv)
    turn_ref[0] = query.T
    turn_ref[1] = key.T
    decays = [
        jnp.where(core == 0, 1.0 - 2.0 ** (-3 - 2 * h), 1.0 - 2.0 ** (-3 - 2 * (h + heads)))
        for h in range(heads)
    ]
    loads[4].wait()
    group = 4
    copies = []
    for s in range(rows):
        for h in range(heads):
            part = slice(h * head, (h + 1) * head)
            q = turn_ref[0, part, s : s + 1]
            k = turn_ref[1, part, s : s + 1]
            new = decays[h] * state_ref[s, h] + k * value[s : s + 1, part]
            new_ref[s, h] = new
            read_ref[s : s + 1, part] = jnp.sum(q * new, axis=0, keepdims=True)
        if s % group == group - 1:
            band = pl.ds(s + 1 - group, group)
            copy = pltpu.make_async_copy(new_ref.at[band], new_hbm.at[band], sem.at[s // group])
            copy.start()
            copies.append(copy)
    outs = []
    for h in range(heads):
        read = read_ref[:, h * head : (h + 1) * head]
        centre = jnp.mean(read, axis=1, keepdims=True)
        spread = jnp.mean(jnp.square(read - centre), axis=1, keepdims=True)
        outs.append(((read - centre) * lax.rsqrt(spread + epsilon)).astype(BF16))
    loads[5].wait()
    mix = jnp.zeros(mix_ref.shape, F32)
    for h in range(heads):
        mix = mix + dot(outs[h], wo[h * head : (h + 1) * head, :])
    mix_ref[...] = mix.astype(BF16)
    for copy in copies:
        copy.wait()


def mixer(core, own, other, gain, wq, wk, wv, wo, state):
    rows, half = own.shape
    heads, head = state.shape[1], state.shape[2]
    vmem = pl.BlockSpec(memory_space=pltpu.VMEM)
    hbm = pl.BlockSpec(memory_space=pl.ANY)
    return pl.pallas_call(
        mixer_kernel,
        name="mixer",
        out_shape=(
            pltpu.VMEM((rows, 2 * half), BF16),
            jax.ShapeDtypeStruct(state.shape, F32),
        ),
        in_specs=[pl.BlockSpec(memory_space=pltpu.SMEM), hbm, vmem, vmem] + [hbm] * 5,
        out_specs=(vmem, hbm),
        scratch_shapes=[
            pltpu.VMEM(own.shape, BF16),
            pltpu.VMEM(wq.shape, BF16),
            pltpu.VMEM(wk.shape, BF16),
            pltpu.VMEM(wv.shape, BF16),
            pltpu.VMEM(wo.shape, BF16),
            pltpu.VMEM(state.shape, F32),
            pltpu.VMEM(state.shape, F32),
            pltpu.VMEM((2, heads * head, rows), F32),
            pltpu.VMEM((rows, heads * head), F32),
            pltpu.SemaphoreType.DMA((rows // 4,)),
            pltpu.SemaphoreType.DMA((6,)),
        ],
    )(
        core.reshape(1), own, in_vmem(other), gain.reshape(1, 2 * half),
        wq, wk, wv, wo, state,
    )


def first_slot(odd, core):
    return jnp.where(odd == core, 0, SLOTS)


def slots_kernel(
    core_ref, z_ref, x_ref, y_ref, mix_ref, mix2_ref, gain_ref, gain2_ref, routes_ref, weights_ref,
    slot_ref, after_ref,
):
    rows, half = x_ref.shape
    core, odd = core_ref[0], z_ref[0] & 1
    here = pl.multiple_of(core * half, half)
    there = pl.multiple_of((1 - core) * half, half)

    def add(ref, at):
        total = mix_ref[:, pl.ds(at, half)].astype(F32) + mix2_ref[:, pl.ds(at, half)].astype(F32)
        return (ref[...].astype(F32) + total).astype(BF16)

    after = add(x_ref, here)
    after_ref[...] = after
    x = after.astype(F32)
    y = add(y_ref, there).astype(F32)
    total = jnp.sum(x * x, axis=1, keepdims=True) + jnp.sum(y * y, axis=1, keepdims=True)
    scale = lax.rsqrt(total / (2 * half) + epsilon)
    x = (x * scale * gain_ref[...]).astype(BF16)
    y = (y * scale * gain2_ref[...]).astype(BF16)

    shape = (EXPERTS * SLOTS, rows)
    slot = iota2(shape, 0)
    expert = divided(slot, 3)
    slot = slot - SLOTS * expert + first_slot(odd, core)
    first = (routes_ref[0:1, :] == expert).astype(F32)
    second = (routes_ref[1:2, :] == expert).astype(F32)
    member = first + second
    earlier = iota2((rows, rows), 0) < iota2((rows, rows), 1)
    place = dot(member.astype(BF16), one_hot(earlier))
    select = jnp.where(place == slot.astype(F32), member, 0.0)
    weight = first * weights_ref[0:1, :].astype(F32) + second * weights_ref[1:2, :].astype(F32)
    weight = jnp.sum(select * weight, axis=1, keepdims=True)
    weight = jnp.broadcast_to(weight, (EXPERTS * SLOTS, 128))
    select = select.astype(BF16)
    x, y = dot(select, x), dot(select, y)
    for k in range(EXPERTS):
        part = slice(k * SLOTS, (k + 1) * SLOTS)
        slot_ref[k, :, pl.ds(here, half)] = x[part].astype(BF16)
        slot_ref[k, :, pl.ds(there, half)] = y[part].astype(BF16)
        slot_ref[k, :, 2 * half :] = weight[part].astype(BF16)


def to_slots(place, own, other, mix, mix2, gain, gain2, routes, route_w):
    rows, half = own.shape
    vmem = pl.BlockSpec(memory_space=pltpu.VMEM)
    return pl.pallas_call(
        slots_kernel,
        name="slots",
        out_shape=(
            pltpu.VMEM((EXPERTS, SLOTS, 2 * half + 128), BF16),
            pltpu.VMEM((rows, half), BF16),
        ),
        in_specs=[pl.BlockSpec(memory_space=pltpu.SMEM)] * 2 + [vmem] * 8,
        out_specs=(vmem, vmem),
    )(
        place[0].reshape(1), place[1].reshape(1), in_vmem(own), in_vmem(other), in_vmem(mix), in_vmem(mix2),
        gain.reshape(1, half), in_vmem(gain2.reshape(1, half)), routes.T, route_w.T,
    )


def home_kernel(z_ref, home_ref, after_ref, routes_ref, out_ref, rows_ref):
    odd = z_ref[0] & 1
    rows = after_ref.shape[0]
    count = home_ref.shape[0]
    for k in range(count):
        rows_ref[k * SLOTS : (k + 1) * SLOTS, :] = home_ref[k].astype(F32)
    shape = (rows, count * SLOTS)
    slot = iota2(shape, 1)
    source = divided(slot, 3)
    expert = source >> 1
    slot = slot - SLOTS * source + first_slot(odd, source & 1)
    member = (routes_ref[:, 0:1] == expert).astype(F32) + (routes_ref[:, 1:2] == expert).astype(F32)
    earlier = iota2((rows, rows), 1) < iota2((rows, rows), 0)
    place = dot(one_hot(earlier), member.astype(BF16))
    select = jnp.where(place == slot.astype(F32), member, 0.0).astype(BF16)
    total = after_ref[...].astype(F32) + dot(select, rows_ref[...].astype(BF16))
    out_ref[...] = total.astype(BF16)


def at_home(place, home, after, routes):
    vmem = pl.BlockSpec(memory_space=pltpu.VMEM)
    return pl.pallas_call(
        home_kernel,
        name="home",
        out_shape=jax.ShapeDtypeStruct(after.shape, BF16),
        in_specs=[pl.BlockSpec(memory_space=pltpu.SMEM)] + [vmem] * 3,
        out_specs=vmem,
        scratch_shapes=[pltpu.VMEM((home.shape[0] * SLOTS, home.shape[2]), F32)],
    )(place[1].reshape(1), in_vmem(home), in_vmem(after), routes)


def layer(
    tokens, state, norm_mix, w_query, w_key, w_value, w_out, norm_ffn, gate_vector,
    dense_gate, dense_up, dense_down, exp_gate, exp_up, exp_down, routes, route_w,
):
    core = lax.axis_index("tp")
    half = tokens.shape[1]
    hidden = dense_gate.shape[1]

    def fill(size):
        return jnp.zeros((size, half), BF16)

    other_x = swap(tokens)
    other_gain = swap(norm_ffn)
    packed = jnp.concatenate(
        [
            dense_gate.T,
            gate_vector[None],
            fill(PAD - hidden - 1),
            dense_up.T,
            fill(PAD - hidden),
            dense_down,
            fill(SENT - 2 * PAD - hidden),
        ],
        axis=0,
    )
    mine = (exp_gate[0].T, exp_up[0].T, exp_down[0])
    theirs = tuple(swap(weights) for weights in mine)

    mix, new_state = mixer(core, tokens, other_x, norm_mix, w_query, w_key, w_value, w_out, state)
    mix2 = swap(mix)
    place = (core, lax.axis_index("ep_0"))
    slot_rows, after = to_slots(
        place, tokens, other_x, mix, mix2, norm_ffn, other_gain, routes, route_w
    )
    at_plane = lax.all_to_all(slot_rows, "ep_0", 0, 0, tiled=True)
    pieces = [packed]
    for shift in (3, -3, -2, 2, 1, -1):
        pieces.append(along_z(packed, shift))
    pieces.append(along_z(pieces[2], -1))
    pieces2 = [swap(piece) for piece in pieces]
    chips = lax.axis_size(PLANE)
    copies = spread(core, at_plane, chips)
    gathered = lax.all_to_all(copies, PLANE, 0, 0, tiled=True)
    partial = experts_and_dense(
        core, gathered.reshape(chips * ROWS, MAIN), mine, theirs, pieces, pieces2, hidden
    )
    back = lax.all_to_all(partial.reshape(chips, ROWS, MAIN), PLANE, 0, 0, tiled=True)
    send = collect(core, back)
    home = lax.all_to_all(send, ("ep_0", "tp"), 0, 0, tiled=True)
    return (at_home(place, home, after, routes), new_state)


def solution(mesh):
    finer = Mesh(mesh.devices.reshape(8, 4, 4, mesh.shape["tp"]), ("ep_0", "ep_1", "ep_2", "tp"))
    in_specs = (
        P(EP, "tp"),
        P(EP, "tp", None, None),
        P(),
        P(None, "tp"),
        P(None, "tp"),
        P(None, "tp"),
        P("tp", None),
        P("tp"),
        P("tp"),
        P("tp", EP),
        P("tp", EP),
        P(EP, "tp"),
        P(EP, None, "tp"),
        P(EP, None, "tp"),
        P(EP, "tp", None),
        P(EP, None),
        P(EP, None),
    )
    out_specs = (P(EP, "tp"), P(EP, "tp", None, None))
    return jax.shard_map(layer, mesh=finer, in_specs=in_specs, out_specs=out_specs, check_vma=False)
```

```python
import jax
import jax.numpy as jnp
from jax import lax
from jax.experimental import pallas as pl
from jax.experimental.pallas import tpu as pltpu
from jax.sharding import Mesh
from jax.sharding import PartitionSpec as P


EXPERTS = 8
SLOTS = 3
EP = ("ep_0", "ep_1", "ep_2")
PLANE = ("ep_1", "ep_2")
PAD = 24
ROWS = 24
LIVE = 20
MAIN = 1792
TAIL = 256
CHUNK = 48

epsilon = 1e-06
F32 = jnp.float32
BF16 = jnp.bfloat16


def swap(value):
    return lax.ppermute(value, "tp", [(0, 1), (1, 0)])


def along_z(value, shift):
    size = lax.axis_size("ep_0")
    return lax.ppermute(value, "ep_0", [(i, (i + shift) % size) for i in range(size)])


def dot(a, b):
    return jnp.dot(a, b, preferred_element_type=F32)


def dot_t(a, b):
    return lax.dot_general(a, b, (((1,), (1,)), ((), ())), preferred_element_type=F32)


def silu(v):
    return v / (1.0 + jnp.exp(-v))


def divided(index, by):
    return {3: (index * 43) >> 7, 5: (index * 13) >> 6, 24: (index * 171) >> 12}[by]


def iota2(shape, dim):
    return lax.broadcasted_iota(jnp.int32, shape, dim)


def one_hot(mask):
    return mask.astype(F32).astype(BF16)


def tail_maps(size, group):
    shape = (size, size)
    row, col = iota2(shape, 0), iota2(shape, 1)
    chunk = divided(row, ROWS)
    place = row - ROWS * chunk
    unpack = (place < LIVE) & (place >> 2 == group) & (col == ROWS * chunk + LIVE + (place & 3))
    pack = (place >= LIVE) & (col == ROWS * chunk + 4 * group + place - LIVE)
    return one_hot(unpack), one_hot(pack)


def branch_kernel(hidden, core_ref, x_ref, *refs):
    weights, pieces = refs[:6], refs[6:-8]
    out_ref, full_ref, up_ref, down_ref, dense_up, dense_down, acc_ref, sem = refs[-8:]
    half = dense_up.shape[2]
    count = len(pieces) // 2
    units = weights[0].shape[0]
    lanes = up_ref.shape[0] // 4
    copies = []

    def fetch(source, into):
        copies.append(pltpu.make_async_copy(source, into, sem.at[len(copies)]))
        copies[-1].start()

    for k, place in enumerate((0, 2, None, 1, 3, None)):
        if place is not None:
            fetch(weights[k], up_ref.at[pl.ds(place * lanes, units)])
    for k, place in ((2, 0), (5, 1)):
        fetch(weights[k], down_ref.at[pl.ds(place * lanes, units)])
    core = core_ref[0]
    here = pl.multiple_of(core * half, half)
    there = pl.multiple_of((1 - core) * half, half)
    total = x_ref.shape[0]
    step = total // 2
    bands = [pl.ds(start, step) for start in range(0, total, step)]
    groups = LIVE // 4
    maps = [tail_maps(step, g) for g in range(groups)]
    lane = iota2((step, 128), 1)
    weight = []
    for band in bands:
        tail = jnp.zeros((step, TAIL), F32)
        w = jnp.zeros((step, 128), F32)
        for g in range(groups):
            tail = tail + dot(maps[g][0], x_ref[band, g * TAIL : (g + 1) * TAIL])
            w = w + jnp.where(
                lane == g, dot(maps[g][0], x_ref[band, groups * TAIL : groups * TAIL + 128]), 0.0
            )
        weight.append(jnp.sum(w, axis=1, keepdims=True))
        full_ref[band, :MAIN] = x_ref[band, :]
        full_ref[band, MAIN:] = tail.astype(BF16)
    w = jnp.concatenate(weight, axis=0)
    for copy in copies:
        copy.wait()
    first = len(copies)
    for k, piece in enumerate(pieces):
        at = (k % count) * CHUNK
        fetch(piece.at[pl.ds(0, CHUNK)], dense_up.at[k // count, pl.ds(at, CHUNK)])
        fetch(piece.at[pl.ds(CHUNK, PAD)], dense_down.at[k // count, pl.ds(at, PAD)])
    for k in range(2):
        down_ref[k * lanes + units : (k + 1) * lanes, :] = jnp.zeros(
            (lanes - units, 2 * half), BF16
        )
    pre = dot_t(full_ref[...], up_ref[...])
    h = w * silu(pre[:, : 2 * lanes]) * pre[:, 2 * lanes :]
    h = jnp.where((iota2((1, 2 * lanes), 1) & (lanes - 1)) < units, h, 0.0).astype(BF16)
    acc_ref[...] = dot(h, down_ref[...])
    for copy in copies[first:]:
        copy.wait()
    for ref in (dense_down.at[0], dense_down.at[1]):
        for k in range(count):
            ref[k * CHUNK + PAD : (k + 1) * CHUNK, :] = jnp.zeros((CHUNK - PAD, half), BF16)
    pre = dot_t(full_ref[:, pl.ds(here, half)], dense_up[0])
    pre = pre + dot_t(full_ref[:, pl.ds(there, half)], dense_up[1])
    logit = pre[:, hidden : hidden + 1]
    up = pltpu.roll(pre, pre.shape[1] - PAD, 1)
    live = (iota2((1, pre.shape[1]), 1) % CHUNK < hidden) & (w > 0.0)
    scale = 0.5 / (1.0 + jnp.exp(-logit))
    hd = jnp.where(live, scale * silu(pre) * up, 0.0).astype(BF16)
    acc_ref[:, pl.ds(here, half)] += dot(hd, dense_down[0])
    acc_ref[:, pl.ds(there, half)] += dot(hd, dense_down[1])
    for band in bands:
        tail = acc_ref[band, MAIN:].astype(BF16)
        for g in range(groups):
            part = slice(g * TAIL, (g + 1) * TAIL)
            out_ref[band, part] = (acc_ref[band, part] + dot(maps[g][1], tail)).astype(BF16)
        out_ref[band, groups * TAIL :] = acc_ref[band, groups * TAIL : MAIN].astype(BF16)


def in_vmem(value):
    return pltpu.with_memory_space_constraint(value, pltpu.VMEM)


def experts_and_dense(core, x, own, other, pieces, pieces2, hidden):
    rows, half = x.shape[0], pieces[0].shape[1]
    width = 2 * half
    vmem = pl.BlockSpec(memory_space=pltpu.VMEM)
    hbm = pl.BlockSpec(memory_space=pl.ANY)
    units = len(pieces) * CHUNK
    return pl.pallas_call(
        lambda *refs: branch_kernel(hidden, *refs),
        name="branch",
        out_shape=pltpu.VMEM((rows, MAIN), BF16),
        in_specs=[pl.BlockSpec(memory_space=pltpu.SMEM), vmem] + [hbm] * (6 + 2 * len(pieces)),
        out_specs=vmem,
        scratch_shapes=[
            pltpu.VMEM((rows, width), BF16),
            pltpu.VMEM((4 * 128, width), BF16),
            pltpu.VMEM((2 * 128, width), BF16),
            pltpu.VMEM((2, units, half), BF16),
            pltpu.VMEM((2, units, half), BF16),
            pltpu.VMEM((rows, width), F32),
            pltpu.SemaphoreType.DMA((6 + 4 * len(pieces),)),
        ],
    )(core.reshape(1), in_vmem(x), *own, *other, *pieces, *pieces2)


def slot_source(core, row):
    pair = divided(row, 5)
    place = row - 5 * pair
    crossed = place + jnp.where(place < SLOTS, SLOTS, -SLOTS)
    return 6 * pair + jnp.where(core == 0, place, crossed)


def spread_kernel(core_ref, x_ref, out_ref, rows_ref):
    core = core_ref[0]
    for k in range(x_ref.shape[0]):
        rows_ref[k * SLOTS : (k + 1) * SLOTS, :] = x_ref[k].astype(F32)
    x = rows_ref[...].astype(BF16)
    width = MAIN + TAIL
    shape = (ROWS, ROWS)
    row, col = iota2(shape, 0), iota2(shape, 1)
    main = dot(one_hot((row < LIVE) & (col == slot_source(core, row))), x[:, :MAIN])
    groups = LIVE // 4
    lane = iota2((ROWS, 128), 1)
    weight = jnp.zeros((ROWS, 128), F32)
    parts = []
    for g in range(groups):
        pick = one_hot((row >= LIVE) & (col == slot_source(core, 4 * g + row - LIVE)))
        parts.append(main[:, g * TAIL : (g + 1) * TAIL] + dot(pick, x[:, MAIN:width]))
        weight = weight + jnp.where(lane == g, dot(pick, x[:, width:]), 0.0)
    parts.append(main[:, groups * TAIL : groups * TAIL + 128] + weight)
    parts.append(main[:, groups * TAIL + 128 :])
    packed = jnp.concatenate(parts, axis=1).astype(BF16)
    for k in range(out_ref.shape[0]):
        out_ref[k] = packed


def spread(core, x, chips):
    vmem = pl.BlockSpec(memory_space=pltpu.VMEM)
    return pl.pallas_call(
        spread_kernel,
        name="spread",
        out_shape=pltpu.VMEM((chips, ROWS, MAIN), BF16),
        in_specs=[pl.BlockSpec(memory_space=pltpu.SMEM), vmem],
        out_specs=vmem,
        scratch_shapes=[pltpu.VMEM((EXPERTS * SLOTS, x.shape[2]), F32)],
    )(core.reshape(1), in_vmem(x))


def collect_kernel(core_ref, x_ref, out_ref, rows_ref):
    core = core_ref[0]
    half = out_ref.shape[2]
    total = x_ref[0].astype(F32)
    for k in range(1, x_ref.shape[0]):
        total = total + x_ref[k].astype(F32)
    total = total.astype(BF16)
    shape = (ROWS, ROWS)
    row, col = iota2(shape, 0), iota2(shape, 1)
    rows_ref[:, :MAIN] = dot(one_hot((col < LIVE) & (row == slot_source(core, col))), total)
    tail = jnp.zeros((ROWS, TAIL), F32)
    for g in range(LIVE // 4):
        pick = one_hot((col >= LIVE) & (row == slot_source(core, 4 * g + col - LIVE)))
        tail = tail + dot(pick, total[:, g * TAIL : (g + 1) * TAIL])
    rows_ref[:, MAIN:] = tail
    for k in range(out_ref.shape[0]):
        at = k // 2 * SLOTS
        part = rows_ref[at : at + SLOTS, k % 2 * half : (k % 2 + 1) * half]
        out_ref[k] = part.astype(BF16)


def collect(core, x):
    vmem = pl.BlockSpec(memory_space=pltpu.VMEM)
    half = (MAIN + TAIL) // 2
    return pl.pallas_call(
        collect_kernel,
        name="collect",
        out_shape=pltpu.VMEM((2 * EXPERTS, SLOTS, half), BF16),
        in_specs=[pl.BlockSpec(memory_space=pltpu.SMEM), vmem],
        out_specs=vmem,
        scratch_shapes=[pltpu.VMEM((ROWS, MAIN + TAIL), F32)],
    )(core.reshape(1), in_vmem(x))


def mixer_kernel(
    core_ref, x_hbm, y_ref, gain_ref, wq_hbm, wk_hbm, wv_hbm, wo_hbm, state_hbm, mix_ref, new_hbm,
    x_ref, wq, wk, wv, wo, state_ref, new_ref, turn_ref, read_ref, sem, load_sem,
):
    rows, half = x_ref.shape
    heads, head = state_ref.shape[1], state_ref.shape[2]
    loads = []
    pairs = ((x_hbm, x_ref), (wq_hbm, wq), (wk_hbm, wk), (wv_hbm, wv), (state_hbm, state_ref), (wo_hbm, wo))
    for k, (source, into) in enumerate(pairs):
        loads.append(pltpu.make_async_copy(source, into, load_sem.at[k]))
    for load in loads[:4]:
        load.start()
    core = core_ref[0]
    here = pl.multiple_of(core * half, half)
    there = pl.multiple_of((1 - core) * half, half)
    loads[0].wait()
    x = x_ref[...].astype(F32)
    y = y_ref[...].astype(F32)
    total = jnp.sum(x * x, axis=1, keepdims=True) + jnp.sum(y * y, axis=1, keepdims=True)
    scale = lax.rsqrt(total / (2 * half) + epsilon)
    x = (x * scale * gain_ref[:, pl.ds(here, half)]).astype(BF16)
    y = (y * scale * gain_ref[:, pl.ds(there, half)]).astype(BF16)

    def project(ref):
        both = dot(x, ref[pl.ds(here, half), :]) + dot(y, ref[pl.ds(there, half), :])
        return both.astype(BF16).astype(F32)

    loads[1].wait()
    for load in loads[4:]:
        load.start()
    query = project(wq)
    loads[2].wait()
    key = project(wk) * head ** (-0.5)
    loads[3].wait()
    value = project(wv)
    turn_ref[0] = query.T
    turn_ref[1] = key.T
    decays = [
        jnp.where(core == 0, 1.0 - 2.0 ** (-3 - 2 * h), 1.0 - 2.0 ** (-3 - 2 * (h + heads)))
        for h in range(heads)
    ]
    loads[4].wait()
    group = 4
    copies = []
    for s in range(rows):
        for h in range(heads):
            part = slice(h * head, (h + 1) * head)
            q = turn_ref[0, part, s : s + 1]
            k = turn_ref[1, part, s : s + 1]
            new = decays[h] * state_ref[s, h] + k * value[s : s + 1, part]
            new_ref[s, h] = new
            read_ref[s : s + 1, part] = jnp.sum(q * new, axis=0, keepdims=True)
        if s % group == group - 1:
            band = pl.ds(s + 1 - group, group)
            copy = pltpu.make_async_copy(new_ref.at[band], new_hbm.at[band], sem.at[s // group])
            copy.start()
            copies.append(copy)
    outs = []
    for h in range(heads):
        read = read_ref[:, h * head : (h + 1) * head]
        centre = jnp.mean(read, axis=1, keepdims=True)
        spread = jnp.mean(jnp.square(read - centre), axis=1, keepdims=True)
        outs.append(((read - centre) * lax.rsqrt(spread + epsilon)).astype(BF16))
    loads[5].wait()
    mix = jnp.zeros(mix_ref.shape, F32)
    for h in range(heads):
        mix = mix + dot(outs[h], wo[h * head : (h + 1) * head, :])
    mix_ref[...] = mix.astype(BF16)
    for copy in copies:
        copy.wait()


def mixer(core, own, other, gain, wq, wk, wv, wo, state):
    rows, half = own.shape
    heads, head = state.shape[1], state.shape[2]
    vmem = pl.BlockSpec(memory_space=pltpu.VMEM)
    hbm = pl.BlockSpec(memory_space=pl.ANY)
    return pl.pallas_call(
        mixer_kernel,
        name="mixer",
        out_shape=(
            pltpu.VMEM((rows, 2 * half), BF16),
            jax.ShapeDtypeStruct(state.shape, F32),
        ),
        in_specs=[pl.BlockSpec(memory_space=pltpu.SMEM), hbm, vmem, vmem] + [hbm] * 5,
        out_specs=(vmem, hbm),
        scratch_shapes=[
            pltpu.VMEM(own.shape, BF16),
            pltpu.VMEM(wq.shape, BF16),
            pltpu.VMEM(wk.shape, BF16),
            pltpu.VMEM(wv.shape, BF16),
            pltpu.VMEM(wo.shape, BF16),
            pltpu.VMEM(state.shape, F32),
            pltpu.VMEM(state.shape, F32),
            pltpu.VMEM((2, heads * head, rows), F32),
            pltpu.VMEM((rows, heads * head), F32),
            pltpu.SemaphoreType.DMA((rows // 4,)),
            pltpu.SemaphoreType.DMA((6,)),
        ],
    )(
        core.reshape(1), own, in_vmem(other), gain.reshape(1, 2 * half),
        wq, wk, wv, wo, state,
    )


def first_slot(odd, core):
    return jnp.where(odd == core, 0, SLOTS)


def slots_kernel(
    core_ref, z_ref, x_ref, y_ref, mix_ref, mix2_ref, gain_ref, gain2_ref, routes_ref, weights_ref,
    slot_ref, after_ref,
):
    rows, half = x_ref.shape
    core, odd = core_ref[0], z_ref[0] & 1
    here = pl.multiple_of(core * half, half)
    there = pl.multiple_of((1 - core) * half, half)

    def add(ref, at):
        total = mix_ref[:, pl.ds(at, half)].astype(F32) + mix2_ref[:, pl.ds(at, half)].astype(F32)
        return (ref[...].astype(F32) + total).astype(BF16)

    after = add(x_ref, here)
    after_ref[...] = after
    x = after.astype(F32)
    y = add(y_ref, there).astype(F32)
    total = jnp.sum(x * x, axis=1, keepdims=True) + jnp.sum(y * y, axis=1, keepdims=True)
    scale = lax.rsqrt(total / (2 * half) + epsilon)
    x = (x * scale * gain_ref[...]).astype(BF16)
    y = (y * scale * gain2_ref[...]).astype(BF16)

    shape = (EXPERTS * SLOTS, rows)
    slot = iota2(shape, 0)
    expert = divided(slot, 3)
    slot = slot - SLOTS * expert + first_slot(odd, core)
    first = (routes_ref[0:1, :] == expert).astype(F32)
    second = (routes_ref[1:2, :] == expert).astype(F32)
    member = first + second
    earlier = iota2((rows, rows), 0) < iota2((rows, rows), 1)
    place = dot(member.astype(BF16), one_hot(earlier))
    select = jnp.where(place == slot.astype(F32), member, 0.0)
    weight = first * weights_ref[0:1, :].astype(F32) + second * weights_ref[1:2, :].astype(F32)
    weight = jnp.sum(select * weight, axis=1, keepdims=True)
    weight = jnp.broadcast_to(weight, (EXPERTS * SLOTS, 128))
    select = select.astype(BF16)
    x, y = dot(select, x), dot(select, y)
    for k in range(EXPERTS):
        part = slice(k * SLOTS, (k + 1) * SLOTS)
        slot_ref[k, :, pl.ds(here, half)] = x[part].astype(BF16)
        slot_ref[k, :, pl.ds(there, half)] = y[part].astype(BF16)
        slot_ref[k, :, 2 * half :] = weight[part].astype(BF16)


def to_slots(place, own, other, mix, mix2, gain, gain2, routes, route_w):
    rows, half = own.shape
    vmem = pl.BlockSpec(memory_space=pltpu.VMEM)
    return pl.pallas_call(
        slots_kernel,
        name="slots",
        out_shape=(
            pltpu.VMEM((EXPERTS, SLOTS, 2 * half + 128), BF16),
            pltpu.VMEM((rows, half), BF16),
        ),
        in_specs=[pl.BlockSpec(memory_space=pltpu.SMEM)] * 2 + [vmem] * 8,
        out_specs=(vmem, vmem),
    )(
        place[0].reshape(1), place[1].reshape(1), in_vmem(own), in_vmem(other), in_vmem(mix), in_vmem(mix2),
        in_vmem(gain.reshape(1, half)), in_vmem(gain2.reshape(1, half)), in_vmem(routes.T),
        in_vmem(route_w.T),
    )


def home_kernel(z_ref, home_ref, after_ref, routes_ref, out_ref, rows_ref):
    odd = z_ref[0] & 1
    rows = after_ref.shape[0]
    count = home_ref.shape[0]
    for k in range(count):
        rows_ref[k * SLOTS : (k + 1) * SLOTS, :] = home_ref[k].astype(F32)
    shape = (rows, count * SLOTS)
    slot = iota2(shape, 1)
    source = divided(slot, 3)
    expert = source >> 1
    slot = slot - SLOTS * source + first_slot(odd, source & 1)
    member = (routes_ref[:, 0:1] == expert).astype(F32) + (routes_ref[:, 1:2] == expert).astype(F32)
    earlier = iota2((rows, rows), 1) < iota2((rows, rows), 0)
    place = dot(one_hot(earlier), member.astype(BF16))
    select = jnp.where(place == slot.astype(F32), member, 0.0).astype(BF16)
    total = after_ref[...].astype(F32) + dot(select, rows_ref[...].astype(BF16))
    out_ref[...] = total.astype(BF16)


def at_home(place, home, after, routes):
    vmem = pl.BlockSpec(memory_space=pltpu.VMEM)
    return pl.pallas_call(
        home_kernel,
        name="home",
        out_shape=jax.ShapeDtypeStruct(after.shape, BF16),
        in_specs=[pl.BlockSpec(memory_space=pltpu.SMEM)] + [vmem] * 3,
        out_specs=vmem,
        scratch_shapes=[pltpu.VMEM((home.shape[0] * SLOTS, home.shape[2]), F32)],
    )(place[1].reshape(1), in_vmem(home), in_vmem(after), in_vmem(routes))


def layer(
    tokens, state, norm_mix, w_query, w_key, w_value, w_out, norm_ffn, gate_vector,
    dense_gate, dense_up, dense_down, exp_gate, exp_up, exp_down, routes, route_w,
):
    core = lax.axis_index("tp")
    half = tokens.shape[1]
    hidden = dense_gate.shape[1]

    def fill(size):
        return jnp.zeros((size, half), BF16)

    other_x = swap(tokens)
    other_gain = swap(norm_ffn)
    packed = jnp.concatenate(
        [
            dense_gate.T,
            gate_vector[None],
            fill(PAD - hidden - 1),
            dense_up.T,
            fill(PAD - hidden),
            dense_down,
            fill(PAD - hidden),
        ],
        axis=0,
    )
    mine = (exp_gate[0].T, exp_up[0].T, exp_down[0])
    theirs = tuple(swap(weights) for weights in mine)

    mix, new_state = mixer(core, tokens, other_x, norm_mix, w_query, w_key, w_value, w_out, state)
    mix2 = swap(mix)
    place = (core, lax.axis_index("ep_0"))
    slot_rows, after = to_slots(
        place, tokens, other_x, mix, mix2, norm_ffn, other_gain, routes, route_w
    )
    at_plane = lax.all_to_all(slot_rows, "ep_0", 0, 0, tiled=True)
    pieces = [packed]
    for shift in (3, -3, -2, 2, 1, -1):
        pieces.append(along_z(packed, shift))
    pieces.append(along_z(pieces[2], -1))
    pieces2 = [swap(piece) for piece in pieces]
    chips = lax.axis_size(PLANE)
    copies = spread(core, at_plane, chips)
    gathered = lax.all_to_all(copies, PLANE, 0, 0, tiled=True)
    partial = experts_and_dense(
        core, gathered.reshape(chips * ROWS, MAIN), mine, theirs, pieces, pieces2, hidden
    )
    back = lax.all_to_all(partial.reshape(chips, ROWS, MAIN), PLANE, 0, 0, tiled=True)
    send = collect(core, back)
    home = lax.all_to_all(send, ("ep_0", "tp"), 0, 0, tiled=True)
    return (at_home(place, home, after, routes), new_state)


def solution(mesh):
    finer = Mesh(mesh.devices.reshape(8, 4, 4, mesh.shape["tp"]), ("ep_0", "ep_1", "ep_2", "tp"))
    in_specs = (
        P(EP, "tp"),
        P(EP, "tp", None, None),
        P(),
        P(None, "tp"),
        P(None, "tp"),
        P(None, "tp"),
        P("tp", None),
        P("tp"),
        P("tp"),
        P("tp", EP),
        P("tp", EP),
        P(EP, "tp"),
        P(EP, None, "tp"),
        P(EP, None, "tp"),
        P(EP, "tp", None),
        P(EP, None),
        P(EP, None),
    )
    out_specs = (P(EP, "tp"), P(EP, "tp", None, None))
    return jax.shard_map(layer, mesh=finer, in_specs=in_specs, out_specs=out_specs, check_vma=False)
```

```python
import jax
import jax.numpy as jnp
from jax import lax
from jax.experimental import pallas as pl
from jax.experimental.pallas import tpu as pltpu
from jax.sharding import Mesh
from jax.sharding import PartitionSpec as P


EXPERTS = 8
SLOTS = 3
EP = ("ep_0", "ep_1", "ep_2")
PLANE = ("ep_1", "ep_2")
PAD = 24
ROWS = 24
LIVE = 20
MAIN = 1792
TAIL = 256
CHUNK = 48

epsilon = 1e-06
F32 = jnp.float32
BF16 = jnp.bfloat16


def swap(value):
    return lax.ppermute(value, "tp", [(0, 1), (1, 0)])


def along_z(value, shift):
    size = lax.axis_size("ep_0")
    return lax.ppermute(value, "ep_0", [(i, (i + shift) % size) for i in range(size)])


def dot(a, b):
    return jnp.dot(a, b, preferred_element_type=F32)


def dot_t(a, b):
    return lax.dot_general(a, b, (((1,), (1,)), ((), ())), preferred_element_type=F32)


def silu(v):
    return v / (1.0 + jnp.exp(-v))


def divided(index, by):
    return {3: (index * 43) >> 7, 5: (index * 13) >> 6, 24: (index * 171) >> 12}[by]


def iota2(shape, dim):
    return lax.broadcasted_iota(jnp.int32, shape, dim)


def one_hot(mask):
    return mask.astype(F32).astype(BF16)


def tail_maps(size, group):
    shape = (size, size)
    row, col = iota2(shape, 0), iota2(shape, 1)
    chunk = divided(row, ROWS)
    place = row - ROWS * chunk
    unpack = (place < LIVE) & (place >> 2 == group) & (col == ROWS * chunk + LIVE + (place & 3))
    pack = (place >= LIVE) & (col == ROWS * chunk + 4 * group + place - LIVE)
    return one_hot(unpack), one_hot(pack)


def branch_kernel(hidden, core_ref, x_ref, *refs):
    weights, pieces = refs[:6], refs[6:-8]
    out_ref, full_ref, up_ref, down_ref, dense_up, dense_down, acc_ref, sem = refs[-8:]
    half = dense_up.shape[2]
    count = len(pieces) // 2
    units = weights[0].shape[0]
    lanes = up_ref.shape[0] // 4
    copies = []

    def fetch(source, into):
        copies.append(pltpu.make_async_copy(source, into, sem.at[len(copies)]))
        copies[-1].start()

    for k, place in enumerate((0, 2, None, 1, 3, None)):
        if place is not None:
            fetch(weights[k], up_ref.at[pl.ds(place * lanes, units)])
    for k, place in ((2, 0), (5, 1)):
        fetch(weights[k], down_ref.at[pl.ds(place * lanes, units)])
    for k, piece in enumerate(pieces):
        at = (k % count) * CHUNK
        fetch(piece.at[pl.ds(0, CHUNK)], dense_up.at[k // count, pl.ds(at, CHUNK)])
        fetch(piece.at[pl.ds(CHUNK, PAD)], dense_down.at[k // count, pl.ds(at, PAD)])
    core = core_ref[0]
    here = pl.multiple_of(core * half, half)
    there = pl.multiple_of((1 - core) * half, half)
    total = x_ref.shape[0]
    step = total // 2
    bands = [pl.ds(start, step) for start in range(0, total, step)]
    groups = LIVE // 4
    maps = [tail_maps(step, g) for g in range(groups)]
    lane = iota2((step, 128), 1)
    weight = []
    for band in bands:
        tail = jnp.zeros((step, TAIL), F32)
        w = jnp.zeros((step, 128), F32)
        for g in range(groups):
            tail = tail + dot(maps[g][0], x_ref[band, g * TAIL : (g + 1) * TAIL])
            w = w + jnp.where(
                lane == g, dot(maps[g][0], x_ref[band, groups * TAIL : groups * TAIL + 128]), 0.0
            )
        weight.append(jnp.sum(w, axis=1, keepdims=True))
        full_ref[band, :MAIN] = x_ref[band, :]
        full_ref[band, MAIN:] = tail.astype(BF16)
    w = jnp.concatenate(weight, axis=0)
    for copy in copies[:6]:
        copy.wait()
    for k in range(2):
        down_ref[k * lanes + units : (k + 1) * lanes, :] = jnp.zeros(
            (lanes - units, 2 * half), BF16
        )
    pre = dot_t(full_ref[...], up_ref[...])
    h = w * silu(pre[:, : 2 * lanes]) * pre[:, 2 * lanes :]
    h = jnp.where((iota2((1, 2 * lanes), 1) & (lanes - 1)) < units, h, 0.0).astype(BF16)
    acc_ref[...] = dot(h, down_ref[...])
    for copy in copies[6:]:
        copy.wait()
    for ref in (dense_down.at[0], dense_down.at[1]):
        for k in range(count):
            ref[k * CHUNK + PAD : (k + 1) * CHUNK, :] = jnp.zeros((CHUNK - PAD, half), BF16)
    pre = dot_t(full_ref[:, pl.ds(here, half)], dense_up[0])
    pre = pre + dot_t(full_ref[:, pl.ds(there, half)], dense_up[1])
    logit = pre[:, hidden : hidden + 1]
    up = pltpu.roll(pre, pre.shape[1] - PAD, 1)
    live = (iota2((1, pre.shape[1]), 1) % CHUNK < hidden) & (w > 0.0)
    scale = 0.5 / (1.0 + jnp.exp(-logit))
    hd = jnp.where(live, scale * silu(pre) * up, 0.0).astype(BF16)
    acc_ref[:, pl.ds(here, half)] += dot(hd, dense_down[0])
    acc_ref[:, pl.ds(there, half)] += dot(hd, dense_down[1])
    for band in bands:
        tail = acc_ref[band, MAIN:].astype(BF16)
        for g in range(groups):
            part = slice(g * TAIL, (g + 1) * TAIL)
            out_ref[band, part] = (acc_ref[band, part] + dot(maps[g][1], tail)).astype(BF16)
        out_ref[band, groups * TAIL :] = acc_ref[band, groups * TAIL : MAIN].astype(BF16)


def in_vmem(value):
    return pltpu.with_memory_space_constraint(value, pltpu.VMEM)


def experts_and_dense(core, x, own, other, pieces, pieces2, hidden):
    rows, half = x.shape[0], pieces[0].shape[1]
    width = 2 * half
    vmem = pl.BlockSpec(memory_space=pltpu.VMEM)
    hbm = pl.BlockSpec(memory_space=pl.ANY)
    units = len(pieces) * CHUNK
    return pl.pallas_call(
        lambda *refs: branch_kernel(hidden, *refs),
        name="branch",
        out_shape=pltpu.VMEM((rows, MAIN), BF16),
        in_specs=[pl.BlockSpec(memory_space=pltpu.SMEM), vmem] + [hbm] * (6 + 2 * len(pieces)),
        out_specs=vmem,
        scratch_shapes=[
            pltpu.VMEM((rows, width), BF16),
            pltpu.VMEM((4 * 128, width), BF16),
            pltpu.VMEM((2 * 128, width), BF16),
            pltpu.VMEM((2, units, half), BF16),
            pltpu.VMEM((2, units, half), BF16),
            pltpu.VMEM((rows, width), F32),
            pltpu.SemaphoreType.DMA((6 + 4 * len(pieces),)),
        ],
    )(core.reshape(1), in_vmem(x), *own, *other, *pieces, *pieces2)


def slot_source(core, row):
    pair = divided(row, 5)
    place = row - 5 * pair
    crossed = place + jnp.where(place < SLOTS, SLOTS, -SLOTS)
    return 6 * pair + jnp.where(core == 0, place, crossed)


def spread_kernel(core_ref, x_ref, out_ref, rows_ref, packed_ref, sem):
    core = core_ref[0]
    for k in range(x_ref.shape[0]):
        rows_ref[k * SLOTS : (k + 1) * SLOTS, :] = x_ref[k].astype(F32)
    x = rows_ref[...].astype(BF16)
    width = MAIN + TAIL
    shape = (ROWS, ROWS)
    row, col = iota2(shape, 0), iota2(shape, 1)
    main = dot(one_hot((row < LIVE) & (col == slot_source(core, row))), x[:, :MAIN])
    groups = LIVE // 4
    lane = iota2((ROWS, 128), 1)
    weight = jnp.zeros((ROWS, 128), F32)
    parts = []
    for g in range(groups):
        pick = one_hot((row >= LIVE) & (col == slot_source(core, 4 * g + row - LIVE)))
        parts.append(main[:, g * TAIL : (g + 1) * TAIL] + dot(pick, x[:, MAIN:width]))
        weight = weight + jnp.where(lane == g, dot(pick, x[:, width:]), 0.0)
    parts.append(main[:, groups * TAIL : groups * TAIL + 128] + weight)
    parts.append(main[:, groups * TAIL + 128 :])
    packed_ref[...] = jnp.concatenate(parts, axis=1).astype(BF16)
    copies = [
        pltpu.make_async_copy(packed_ref, out_ref.at[k], sem.at[k])
        for k in range(out_ref.shape[0])
    ]
    for copy in copies:
        copy.start()
    for copy in copies:
        copy.wait()


def spread(core, x, chips):
    vmem = pl.BlockSpec(memory_space=pltpu.VMEM)
    return pl.pallas_call(
        spread_kernel,
        name="spread",
        out_shape=jax.ShapeDtypeStruct((chips, ROWS, MAIN), BF16),
        in_specs=[pl.BlockSpec(memory_space=pltpu.SMEM), vmem],
        out_specs=pl.BlockSpec(memory_space=pl.ANY),
        scratch_shapes=[
            pltpu.VMEM((EXPERTS * SLOTS, x.shape[2]), F32),
            pltpu.VMEM((ROWS, MAIN), BF16),
            pltpu.SemaphoreType.DMA((chips,)),
        ],
    )(core.reshape(1), in_vmem(x))


def collect_kernel(core_ref, x_ref, out_ref, rows_ref):
    core = core_ref[0]
    half = out_ref.shape[2]
    total = x_ref[0].astype(F32)
    for k in range(1, x_ref.shape[0]):
        total = total + x_ref[k].astype(F32)
    total = total.astype(BF16)
    shape = (ROWS, ROWS)
    row, col = iota2(shape, 0), iota2(shape, 1)
    rows_ref[:, :MAIN] = dot(one_hot((col < LIVE) & (row == slot_source(core, col))), total)
    tail = jnp.zeros((ROWS, TAIL), F32)
    for g in range(LIVE // 4):
        pick = one_hot((col >= LIVE) & (row == slot_source(core, 4 * g + col - LIVE)))
        tail = tail + dot(pick, total[:, g * TAIL : (g + 1) * TAIL])
    rows_ref[:, MAIN:] = tail
    for k in range(out_ref.shape[0]):
        at = k // 2 * SLOTS
        part = rows_ref[at : at + SLOTS, k % 2 * half : (k % 2 + 1) * half]
        out_ref[k] = part.astype(BF16)


def collect(core, x):
    vmem = pl.BlockSpec(memory_space=pltpu.VMEM)
    half = (MAIN + TAIL) // 2
    return pl.pallas_call(
        collect_kernel,
        name="collect",
        out_shape=pltpu.VMEM((2 * EXPERTS, SLOTS, half), BF16),
        in_specs=[pl.BlockSpec(memory_space=pltpu.SMEM), vmem],
        out_specs=vmem,
        scratch_shapes=[pltpu.VMEM((ROWS, MAIN + TAIL), F32)],
    )(core.reshape(1), in_vmem(x))


def mixer_kernel(
    core_ref, x_hbm, y_ref, gain_ref, wq_hbm, wk_hbm, wv_hbm, wo_hbm, state_hbm, mix_ref, new_hbm,
    x_ref, wq, wk, wv, wo, state_ref, new_ref, turn_ref, read_ref, sem, load_sem,
):
    rows, half = x_ref.shape
    heads, head = state_ref.shape[1], state_ref.shape[2]
    loads = []
    pairs = ((x_hbm, x_ref), (wq_hbm, wq), (wk_hbm, wk), (wv_hbm, wv), (state_hbm, state_ref), (wo_hbm, wo))
    for k, (source, into) in enumerate(pairs):
        loads.append(pltpu.make_async_copy(source, into, load_sem.at[k]))
        loads[-1].start()
    core = core_ref[0]
    here = pl.multiple_of(core * half, half)
    there = pl.multiple_of((1 - core) * half, half)
    loads[0].wait()
    x = x_ref[...].astype(F32)
    y = y_ref[...].astype(F32)
    total = jnp.sum(x * x, axis=1, keepdims=True) + jnp.sum(y * y, axis=1, keepdims=True)
    scale = lax.rsqrt(total / (2 * half) + epsilon)
    x = (x * scale * gain_ref[:, pl.ds(here, half)]).astype(BF16)
    y = (y * scale * gain_ref[:, pl.ds(there, half)]).astype(BF16)

    def project(ref):
        both = dot(x, ref[pl.ds(here, half), :]) + dot(y, ref[pl.ds(there, half), :])
        return both.astype(BF16).astype(F32)

    loads[1].wait()
    query = project(wq)
    loads[2].wait()
    key = project(wk) * head ** (-0.5)
    loads[3].wait()
    value = project(wv)
    turn_ref[0] = query.T
    turn_ref[1] = key.T
    decays = [
        jnp.where(core == 0, 1.0 - 2.0 ** (-3 - 2 * h), 1.0 - 2.0 ** (-3 - 2 * (h + heads)))
        for h in range(heads)
    ]
    loads[4].wait()
    group = 4
    copies = []
    for s in range(rows):
        for h in range(heads):
            part = slice(h * head, (h + 1) * head)
            q = turn_ref[0, part, s : s + 1]
            k = turn_ref[1, part, s : s + 1]
            new = decays[h] * state_ref[s, h] + k * value[s : s + 1, part]
            new_ref[s, h] = new
            read_ref[s : s + 1, part] = jnp.sum(q * new, axis=0, keepdims=True)
        if s % group == group - 1:
            band = pl.ds(s + 1 - group, group)
            copy = pltpu.make_async_copy(new_ref.at[band], new_hbm.at[band], sem.at[s // group])
            copy.start()
            copies.append(copy)
    outs = []
    for h in range(heads):
        read = read_ref[:, h * head : (h + 1) * head]
        centre = jnp.mean(read, axis=1, keepdims=True)
        spread = jnp.mean(jnp.square(read - centre), axis=1, keepdims=True)
        outs.append(((read - centre) * lax.rsqrt(spread + epsilon)).astype(BF16))
    loads[5].wait()
    mix = jnp.zeros(mix_ref.shape, F32)
    for h in range(heads):
        mix = mix + dot(outs[h], wo[h * head : (h + 1) * head, :])
    mix_ref[...] = mix.astype(BF16)
    for copy in copies:
        copy.wait()


def mixer(core, own, other, gain, wq, wk, wv, wo, state):
    rows, half = own.shape
    heads, head = state.shape[1], state.shape[2]
    vmem = pl.BlockSpec(memory_space=pltpu.VMEM)
    hbm = pl.BlockSpec(memory_space=pl.ANY)
    return pl.pallas_call(
        mixer_kernel,
        name="mixer",
        out_shape=(
            pltpu.VMEM((rows, 2 * half), BF16),
            jax.ShapeDtypeStruct(state.shape, F32),
        ),
        in_specs=[pl.BlockSpec(memory_space=pltpu.SMEM), hbm, vmem, vmem] + [hbm] * 5,
        out_specs=(vmem, hbm),
        scratch_shapes=[
            pltpu.VMEM(own.shape, BF16),
            pltpu.VMEM(wq.shape, BF16),
            pltpu.VMEM(wk.shape, BF16),
            pltpu.VMEM(wv.shape, BF16),
            pltpu.VMEM(wo.shape, BF16),
            pltpu.VMEM(state.shape, F32),
            pltpu.VMEM(state.shape, F32),
            pltpu.VMEM((2, heads * head, rows), F32),
            pltpu.VMEM((rows, heads * head), F32),
            pltpu.SemaphoreType.DMA((rows // 4,)),
            pltpu.SemaphoreType.DMA((6,)),
        ],
    )(
        core.reshape(1), own, in_vmem(other), gain.reshape(1, 2 * half),
        wq, wk, wv, wo, state,
    )


def first_slot(odd, core):
    return jnp.where(odd == core, 0, SLOTS)


def slots_kernel(
    core_ref, z_ref, x_ref, y_ref, mix_ref, mix2_ref, gain_ref, gain2_ref, routes_ref, weights_ref,
    slot_ref, after_ref,
):
    rows, half = x_ref.shape
    core, odd = core_ref[0], z_ref[0] & 1
    here = pl.multiple_of(core * half, half)
    there = pl.multiple_of((1 - core) * half, half)

    def add(ref, at):
        total = mix_ref[:, pl.ds(at, half)].astype(F32) + mix2_ref[:, pl.ds(at, half)].astype(F32)
        return (ref[...].astype(F32) + total).astype(BF16)

    after = add(x_ref, here)
    after_ref[...] = after
    x = after.astype(F32)
    y = add(y_ref, there).astype(F32)
    total = jnp.sum(x * x, axis=1, keepdims=True) + jnp.sum(y * y, axis=1, keepdims=True)
    scale = lax.rsqrt(total / (2 * half) + epsilon)
    x = (x * scale * gain_ref[...]).astype(BF16)
    y = (y * scale * gain2_ref[...]).astype(BF16)

    shape = (EXPERTS * SLOTS, rows)
    slot = iota2(shape, 0)
    expert = divided(slot, 3)
    slot = slot - SLOTS * expert + first_slot(odd, core)
    first = (routes_ref[0:1, :] == expert).astype(F32)
    second = (routes_ref[1:2, :] == expert).astype(F32)
    member = first + second
    earlier = iota2((rows, rows), 0) < iota2((rows, rows), 1)
    place = dot(member.astype(BF16), one_hot(earlier))
    select = jnp.where(place == slot.astype(F32), member, 0.0)
    weight = first * weights_ref[0:1, :].astype(F32) + second * weights_ref[1:2, :].astype(F32)
    weight = jnp.sum(select * weight, axis=1, keepdims=True)
    weight = jnp.broadcast_to(weight, (EXPERTS * SLOTS, 128))
    select = select.astype(BF16)
    x, y = dot(select, x), dot(select, y)
    for k in range(EXPERTS):
        part = slice(k * SLOTS, (k + 1) * SLOTS)
        slot_ref[k, :, pl.ds(here, half)] = x[part].astype(BF16)
        slot_ref[k, :, pl.ds(there, half)] = y[part].astype(BF16)
        slot_ref[k, :, 2 * half :] = weight[part].astype(BF16)


def to_slots(place, own, other, mix, mix2, gain, gain2, routes, route_w):
    rows, half = own.shape
    vmem = pl.BlockSpec(memory_space=pltpu.VMEM)
    return pl.pallas_call(
        slots_kernel,
        name="slots",
        out_shape=(
            pltpu.VMEM((EXPERTS, SLOTS, 2 * half + 128), BF16),
            pltpu.VMEM((rows, half), BF16),
        ),
        in_specs=[pl.BlockSpec(memory_space=pltpu.SMEM)] * 2 + [vmem] * 8,
        out_specs=(vmem, vmem),
    )(
        place[0].reshape(1), place[1].reshape(1), in_vmem(own), in_vmem(other), in_vmem(mix), in_vmem(mix2),
        in_vmem(gain.reshape(1, half)), in_vmem(gain2.reshape(1, half)), in_vmem(routes.T),
        in_vmem(route_w.T),
    )


def pick_kernel(z_ref, routes_ref, pick_ref):
    odd = z_ref[0] & 1
    shape = pick_ref.shape
    rows = shape[0]
    slot = iota2(shape, 1)
    source = divided(slot, 3)
    expert = source >> 1
    slot = slot - SLOTS * source + first_slot(odd, source & 1)
    member = (routes_ref[:, 0:1] == expert).astype(F32) + (routes_ref[:, 1:2] == expert).astype(F32)
    earlier = iota2((rows, rows), 1) < iota2((rows, rows), 0)
    place = dot(one_hot(earlier), member.astype(BF16))
    pick_ref[...] = jnp.where(place == slot.astype(F32), member, 0.0).astype(BF16)


def to_pick(z, routes):
    vmem = pl.BlockSpec(memory_space=pltpu.VMEM)
    return pl.pallas_call(
        pick_kernel,
        name="pick",
        out_shape=pltpu.VMEM((routes.shape[0], 2 * EXPERTS * SLOTS), BF16),
        in_specs=[pl.BlockSpec(memory_space=pltpu.SMEM), vmem],
        out_specs=vmem,
    )(z.reshape(1), in_vmem(routes))


def home_kernel(home_ref, after_ref, pick_ref, out_ref, rows_ref):
    for k in range(home_ref.shape[0]):
        rows_ref[k * SLOTS : (k + 1) * SLOTS, :] = home_ref[k].astype(F32)
    total = after_ref[...].astype(F32) + dot(pick_ref[...], rows_ref[...].astype(BF16))
    out_ref[...] = total.astype(BF16)


def at_home(home, after, pick):
    vmem = pl.BlockSpec(memory_space=pltpu.VMEM)
    return pl.pallas_call(
        home_kernel,
        name="home",
        out_shape=jax.ShapeDtypeStruct(after.shape, BF16),
        in_specs=[vmem] * 3,
        out_specs=vmem,
        scratch_shapes=[pltpu.VMEM((home.shape[0] * SLOTS, home.shape[2]), F32)],
    )(in_vmem(home), in_vmem(after), in_vmem(pick))


def layer(
    tokens, state, norm_mix, w_query, w_key, w_value, w_out, norm_ffn, gate_vector,
    dense_gate, dense_up, dense_down, exp_gate, exp_up, exp_down, routes, route_w,
):
    core = lax.axis_index("tp")
    half = tokens.shape[1]
    hidden = dense_gate.shape[1]

    def fill(size):
        return jnp.zeros((size, half), BF16)

    other_x = swap(tokens)
    other_gain = swap(norm_ffn)
    packed = jnp.concatenate(
        [
            dense_gate.T,
            gate_vector[None],
            fill(PAD - hidden - 1),
            dense_up.T,
            fill(PAD - hidden),
            dense_down,
            fill(PAD - hidden),
        ],
        axis=0,
    )
    mine = (exp_gate[0].T, exp_up[0].T, exp_down[0])
    theirs = tuple(swap(weights) for weights in mine)

    mix, new_state = mixer(core, tokens, other_x, norm_mix, w_query, w_key, w_value, w_out, state)
    mix2 = swap(mix)
    place = (core, lax.axis_index("ep_0"))
    slot_rows, after = to_slots(
        place, tokens, other_x, mix, mix2, norm_ffn, other_gain, routes, route_w
    )
    at_plane = lax.all_to_all(slot_rows, "ep_0", 0, 0, tiled=True)
    pieces = [packed]
    for shift in (3, -3, -2, 2, 1, -1):
        pieces.append(along_z(packed, shift))
    pieces.append(along_z(pieces[2], -1))
    pieces2 = [swap(piece) for piece in pieces]
    chips = lax.axis_size(PLANE)
    copies = spread(core, at_plane, chips)
    gathered = lax.all_to_all(copies, PLANE, 0, 0, tiled=True)
    partial = experts_and_dense(
        core, gathered.reshape(chips * ROWS, MAIN), mine, theirs, pieces, pieces2, hidden
    )
    back = lax.all_to_all(partial.reshape(chips, ROWS, MAIN), PLANE, 0, 0, tiled=True)
    send = collect(core, back)
    home = lax.all_to_all(send, ("ep_0", "tp"), 0, 0, tiled=True)
    return (at_home(home, after, to_pick(place[1], routes)), new_state)


def solution(mesh):
    finer = Mesh(mesh.devices.reshape(8, 4, 4, mesh.shape["tp"]), ("ep_0", "ep_1", "ep_2", "tp"))
    in_specs = (
        P(EP, "tp"),
        P(EP, "tp", None, None),
        P(),
        P(None, "tp"),
        P(None, "tp"),
        P(None, "tp"),
        P("tp", None),
        P("tp"),
        P("tp"),
        P("tp", EP),
        P("tp", EP),
        P(EP, "tp"),
        P(EP, None, "tp"),
        P(EP, None, "tp"),
        P(EP, "tp", None),
        P(EP, None),
        P(EP, None),
    )
    out_specs = (P(EP, "tp"), P(EP, "tp", None, None))
    return jax.shard_map(layer, mesh=finer, in_specs=in_specs, out_specs=out_specs, check_vma=False)
```

```python
import jax
import jax.numpy as jnp
from jax import lax
from jax.experimental import pallas as pl
from jax.experimental.pallas import tpu as pltpu
from jax.sharding import Mesh
from jax.sharding import PartitionSpec as P


EXPERTS = 8
SLOTS = 3
EP = ("ep_0", "ep_1", "ep_2")
PLANE = ("ep_1", "ep_2")
PAD = 24
ROWS = 24
LIVE = 20
MAIN = 1792
TAIL = 256
CHUNK = 48

epsilon = 1e-06
F32 = jnp.float32
BF16 = jnp.bfloat16


def swap(value):
    return lax.ppermute(value, "tp", [(0, 1), (1, 0)])


def along_z(value, shift):
    size = lax.axis_size("ep_0")
    return lax.ppermute(value, "ep_0", [(i, (i + shift) % size) for i in range(size)])


def dot(a, b):
    return jnp.dot(a, b, preferred_element_type=F32)


def dot_t(a, b):
    return lax.dot_general(a, b, (((1,), (1,)), ((), ())), preferred_element_type=F32)


def silu(v):
    return v / (1.0 + jnp.exp(-v))


def divided(index, by):
    return {3: (index * 43) >> 7, 5: (index * 13) >> 6, 24: (index * 171) >> 12}[by]


def iota2(shape, dim):
    return lax.broadcasted_iota(jnp.int32, shape, dim)


def one_hot(mask):
    return mask.astype(F32).astype(BF16)


def tail_maps(size, group):
    shape = (size, size)
    row, col = iota2(shape, 0), iota2(shape, 1)
    chunk = divided(row, ROWS)
    place = row - ROWS * chunk
    unpack = (place < LIVE) & (place >> 2 == group) & (col == ROWS * chunk + LIVE + (place & 3))
    pack = (place >= LIVE) & (col == ROWS * chunk + 4 * group + place - LIVE)
    return one_hot(unpack), one_hot(pack)


def branch_kernel(hidden, core_ref, x_ref, *refs):
    weights, pieces = refs[:6], refs[6:-8]
    out_ref, full_ref, up_ref, down_ref, dense_up, dense_down, acc_ref, sem = refs[-8:]
    half = dense_up.shape[2]
    count = len(pieces) // 2
    units = weights[0].shape[0]
    lanes = up_ref.shape[0] // 4
    copies = []

    def fetch(source, into):
        copies.append(pltpu.make_async_copy(source, into, sem.at[len(copies)]))
        copies[-1].start()

    for k, place in enumerate((0, 2, None, 1, 3, None)):
        if place is not None:
            fetch(weights[k], up_ref.at[pl.ds(place * lanes, units)])
    for k, place in ((2, 0), (5, 1)):
        fetch(weights[k], down_ref.at[pl.ds(place * lanes, units)])
    for k, piece in enumerate(pieces):
        at = (k % count) * CHUNK
        fetch(piece.at[pl.ds(0, CHUNK)], dense_up.at[k // count, pl.ds(at, CHUNK)])
        fetch(piece.at[pl.ds(CHUNK, PAD)], dense_down.at[k // count, pl.ds(at, PAD)])
    core = core_ref[0]
    here = pl.multiple_of(core * half, half)
    there = pl.multiple_of((1 - core) * half, half)
    total = x_ref.shape[0]
    step = total // 2
    bands = [pl.ds(start, step) for start in range(0, total, step)]
    groups = LIVE // 4
    maps = [tail_maps(step, g) for g in range(groups)]
    lane = iota2((step, 128), 1)
    weight = []
    for band in bands:
        tail = jnp.zeros((step, TAIL), F32)
        w = jnp.zeros((step, 128), F32)
        for g in range(groups):
            tail = tail + dot(maps[g][0], x_ref[band, g * TAIL : (g + 1) * TAIL])
            w = w + jnp.where(
                lane == g, dot(maps[g][0], x_ref[band, groups * TAIL : groups * TAIL + 128]), 0.0
            )
        weight.append(jnp.sum(w, axis=1, keepdims=True))
        full_ref[band, :MAIN] = x_ref[band, :]
        full_ref[band, MAIN:] = tail.astype(BF16)
    w = jnp.concatenate(weight, axis=0)
    for copy in copies[:6]:
        copy.wait()
    for k in range(2):
        down_ref[k * lanes + units : (k + 1) * lanes, :] = jnp.zeros(
            (lanes - units, 2 * half), BF16
        )
    pre = dot_t(full_ref[...], up_ref[...])
    h = w * silu(pre[:, : 2 * lanes]) * pre[:, 2 * lanes :]
    h = jnp.where((iota2((1, 2 * lanes), 1) & (lanes - 1)) < units, h, 0.0).astype(BF16)
    acc_ref[...] = dot(h, down_ref[...])
    for copy in copies[6:]:
        copy.wait()
    for ref in (dense_down.at[0], dense_down.at[1]):
        for k in range(count):
            ref[k * CHUNK + PAD : (k + 1) * CHUNK, :] = jnp.zeros((CHUNK - PAD, half), BF16)
    pre = dot_t(full_ref[:, pl.ds(here, half)], dense_up[0])
    pre = pre + dot_t(full_ref[:, pl.ds(there, half)], dense_up[1])
    logit = pre[:, hidden : hidden + 1]
    up = pltpu.roll(pre, pre.shape[1] - PAD, 1)
    live = (iota2((1, pre.shape[1]), 1) % CHUNK < hidden) & (w > 0.0)
    scale = 0.5 / (1.0 + jnp.exp(-logit))
    hd = jnp.where(live, scale * silu(pre) * up, 0.0).astype(BF16)
    acc_ref[:, pl.ds(here, half)] += dot(hd, dense_down[0])
    acc_ref[:, pl.ds(there, half)] += dot(hd, dense_down[1])
    for band in bands:
        tail = acc_ref[band, MAIN:].astype(BF16)
        for g in range(groups):
            part = slice(g * TAIL, (g + 1) * TAIL)
            out_ref[band, part] = (acc_ref[band, part] + dot(maps[g][1], tail)).astype(BF16)
        out_ref[band, groups * TAIL :] = acc_ref[band, groups * TAIL : MAIN].astype(BF16)


def in_vmem(value):
    return pltpu.with_memory_space_constraint(value, pltpu.VMEM)


def experts_and_dense(core, x, own, other, pieces, pieces2, hidden):
    rows, half = x.shape[0], pieces[0].shape[1]
    width = 2 * half
    vmem = pl.BlockSpec(memory_space=pltpu.VMEM)
    hbm = pl.BlockSpec(memory_space=pl.ANY)
    units = len(pieces) * CHUNK
    return pl.pallas_call(
        lambda *refs: branch_kernel(hidden, *refs),
        name="branch",
        out_shape=pltpu.VMEM((rows, MAIN), BF16),
        in_specs=[pl.BlockSpec(memory_space=pltpu.SMEM), vmem] + [hbm] * (6 + 2 * len(pieces)),
        out_specs=vmem,
        scratch_shapes=[
            pltpu.VMEM((rows, width), BF16),
            pltpu.VMEM((4 * 128, width), BF16),
            pltpu.VMEM((2 * 128, width), BF16),
            pltpu.VMEM((2, units, half), BF16),
            pltpu.VMEM((2, units, half), BF16),
            pltpu.VMEM((rows, width), F32),
            pltpu.SemaphoreType.DMA((6 + 4 * len(pieces),)),
        ],
    )(core.reshape(1), in_vmem(x), *own, *other, *pieces, *pieces2)


def slot_source(core, row):
    pair = divided(row, 5)
    place = row - 5 * pair
    crossed = place + jnp.where(place < SLOTS, SLOTS, -SLOTS)
    return 6 * pair + jnp.where(core == 0, place, crossed)


def spread_kernel(core_ref, x_ref, out_ref, rows_ref):
    core = core_ref[0]
    for k in range(x_ref.shape[0]):
        rows_ref[k * SLOTS : (k + 1) * SLOTS, :] = x_ref[k].astype(F32)
    x = rows_ref[...].astype(BF16)
    width = MAIN + TAIL
    shape = (ROWS, ROWS)
    row, col = iota2(shape, 0), iota2(shape, 1)
    main = dot(one_hot((row < LIVE) & (col == slot_source(core, row))), x[:, :MAIN])
    groups = LIVE // 4
    lane = iota2((ROWS, 128), 1)
    weight = jnp.zeros((ROWS, 128), F32)
    parts = []
    for g in range(groups):
        pick = one_hot((row >= LIVE) & (col == slot_source(core, 4 * g + row - LIVE)))
        parts.append(main[:, g * TAIL : (g + 1) * TAIL] + dot(pick, x[:, MAIN:width]))
        weight = weight + jnp.where(lane == g, dot(pick, x[:, width:]), 0.0)
    parts.append(main[:, groups * TAIL : groups * TAIL + 128] + weight)
    parts.append(main[:, groups * TAIL + 128 :])
    packed = jnp.concatenate(parts, axis=1).astype(BF16)
    for k in range(out_ref.shape[0]):
        out_ref[k] = packed


def spread(core, x, chips):
    vmem = pl.BlockSpec(memory_space=pltpu.VMEM)
    return pl.pallas_call(
        spread_kernel,
        name="spread",
        out_shape=pltpu.VMEM((chips, ROWS, MAIN), BF16),
        in_specs=[pl.BlockSpec(memory_space=pltpu.SMEM), vmem],
        out_specs=vmem,
        scratch_shapes=[pltpu.VMEM((EXPERTS * SLOTS, x.shape[2]), F32)],
    )(core.reshape(1), in_vmem(x))


def collect_kernel(core_ref, x_ref, out_ref, rows_ref):
    core = core_ref[0]
    half = out_ref.shape[2]
    total = x_ref[0].astype(F32)
    for k in range(1, x_ref.shape[0]):
        total = total + x_ref[k].astype(F32)
    total = total.astype(BF16)
    shape = (ROWS, ROWS)
    row, col = iota2(shape, 0), iota2(shape, 1)
    rows_ref[:, :MAIN] = dot(one_hot((col < LIVE) & (row == slot_source(core, col))), total)
    tail = jnp.zeros((ROWS, TAIL), F32)
    for g in range(LIVE // 4):
        pick = one_hot((col >= LIVE) & (row == slot_source(core, 4 * g + col - LIVE)))
        tail = tail + dot(pick, total[:, g * TAIL : (g + 1) * TAIL])
    rows_ref[:, MAIN:] = tail
    for k in range(out_ref.shape[0]):
        at = k // 2 * SLOTS
        part = rows_ref[at : at + SLOTS, k % 2 * half : (k % 2 + 1) * half]
        out_ref[k] = part.astype(BF16)


def collect(core, x):
    vmem = pl.BlockSpec(memory_space=pltpu.VMEM)
    half = (MAIN + TAIL) // 2
    return pl.pallas_call(
        collect_kernel,
        name="collect",
        out_shape=pltpu.VMEM((2 * EXPERTS, SLOTS, half), BF16),
        in_specs=[pl.BlockSpec(memory_space=pltpu.SMEM), vmem],
        out_specs=vmem,
        scratch_shapes=[pltpu.VMEM((ROWS, MAIN + TAIL), F32)],
    )(core.reshape(1), in_vmem(x))


def mixer_kernel(
    core_ref, x_hbm, y_ref, gain_ref, wq_hbm, wk_hbm, wv_hbm, wo_hbm, state_hbm, mix_ref, new_hbm,
    x_ref, wq, wk, wv, wo, state_ref, new_ref, turn_ref, read_ref, sem, load_sem,
):
    rows, half = x_ref.shape
    heads, head = state_ref.shape[1], state_ref.shape[2]
    loads = []
    pairs = ((x_hbm, x_ref), (wq_hbm, wq), (wk_hbm, wk), (wv_hbm, wv), (state_hbm, state_ref), (wo_hbm, wo))
    for k, (source, into) in enumerate(pairs):
        loads.append(pltpu.make_async_copy(source, into, load_sem.at[k]))
        loads[-1].start()
    core = core_ref[0]
    here = pl.multiple_of(core * half, half)
    there = pl.multiple_of((1 - core) * half, half)
    loads[0].wait()
    x = x_ref[...].astype(F32)
    y = y_ref[...].astype(F32)
    total = jnp.sum(x * x, axis=1, keepdims=True) + jnp.sum(y * y, axis=1, keepdims=True)
    scale = lax.rsqrt(total / (2 * half) + epsilon)
    x = (x * scale * gain_ref[:, pl.ds(here, half)]).astype(BF16)
    y = (y * scale * gain_ref[:, pl.ds(there, half)]).astype(BF16)

    def project(ref):
        both = dot(x, ref[pl.ds(here, half), :]) + dot(y, ref[pl.ds(there, half), :])
        return both.astype(BF16).astype(F32)

    loads[1].wait()
    query = project(wq)
    loads[2].wait()
    key = project(wk) * head ** (-0.5)
    loads[3].wait()
    value = project(wv)
    turn_ref[0] = query.T
    turn_ref[1] = key.T
    decays = [
        jnp.where(core == 0, 1.0 - 2.0 ** (-3 - 2 * h), 1.0 - 2.0 ** (-3 - 2 * (h + heads)))
        for h in range(heads)
    ]
    loads[4].wait()
    group = 4
    copies = []
    for s in range(rows):
        for h in range(heads):
            part = slice(h * head, (h + 1) * head)
            q = turn_ref[0, part, s : s + 1]
            k = turn_ref[1, part, s : s + 1]
            new = decays[h] * state_ref[s, h] + k * value[s : s + 1, part]
            new_ref[s, h] = new
            read_ref[s : s + 1, part] = jnp.sum(q * new, axis=0, keepdims=True)
        if s % group == group - 1:
            band = pl.ds(s + 1 - group, group)
            copy = pltpu.make_async_copy(new_ref.at[band], new_hbm.at[band], sem.at[s // group])
            copy.start()
            copies.append(copy)
    outs = []
    for h in range(heads):
        read = read_ref[:, h * head : (h + 1) * head]
        centre = jnp.mean(read, axis=1, keepdims=True)
        spread = jnp.mean(jnp.square(read - centre), axis=1, keepdims=True)
        outs.append(((read - centre) * lax.rsqrt(spread + epsilon)).astype(BF16))
    loads[5].wait()
    mix = jnp.zeros(mix_ref.shape, F32)
    for h in range(heads):
        mix = mix + dot(outs[h], wo[h * head : (h + 1) * head, :])
    mix_ref[...] = mix.astype(BF16)
    for copy in copies:
        copy.wait()


def mixer(core, own, other, gain, wq, wk, wv, wo, state):
    rows, half = own.shape
    heads, head = state.shape[1], state.shape[2]
    vmem = pl.BlockSpec(memory_space=pltpu.VMEM)
    hbm = pl.BlockSpec(memory_space=pl.ANY)
    return pl.pallas_call(
        mixer_kernel,
        name="mixer",
        out_shape=(
            pltpu.VMEM((rows, 2 * half), BF16),
            jax.ShapeDtypeStruct(state.shape, F32),
        ),
        in_specs=[pl.BlockSpec(memory_space=pltpu.SMEM), hbm, vmem, vmem] + [hbm] * 5,
        out_specs=(vmem, hbm),
        scratch_shapes=[
            pltpu.VMEM(own.shape, BF16),
            pltpu.VMEM(wq.shape, BF16),
            pltpu.VMEM(wk.shape, BF16),
            pltpu.VMEM(wv.shape, BF16),
            pltpu.VMEM(wo.shape, BF16),
            pltpu.VMEM(state.shape, F32),
            pltpu.VMEM(state.shape, F32),
            pltpu.VMEM((2, heads * head, rows), F32),
            pltpu.VMEM((rows, heads * head), F32),
            pltpu.SemaphoreType.DMA((rows // 4,)),
            pltpu.SemaphoreType.DMA((6,)),
        ],
    )(
        core.reshape(1), own, in_vmem(other), gain.reshape(1, 2 * half),
        wq, wk, wv, wo, state,
    )


def first_slot(odd, core):
    return jnp.where(odd == core, 0, SLOTS)


def slots_kernel(
    core_ref, z_ref, x_ref, y_ref, mix_ref, mix2_ref, gain_ref, gain2_ref, routes_ref, weights_ref,
    slot_ref, after_ref,
):
    rows, half = x_ref.shape
    core, odd = core_ref[0], z_ref[0] & 1
    here = pl.multiple_of(core * half, half)
    there = pl.multiple_of((1 - core) * half, half)

    def add(ref, at):
        total = mix_ref[:, pl.ds(at, half)].astype(F32) + mix2_ref[:, pl.ds(at, half)].astype(F32)
        return (ref[...].astype(F32) + total).astype(BF16)

    after = add(x_ref, here)
    after_ref[...] = after
    x = after.astype(F32)
    y = add(y_ref, there).astype(F32)
    total = jnp.sum(x * x, axis=1, keepdims=True) + jnp.sum(y * y, axis=1, keepdims=True)
    scale = lax.rsqrt(total / (2 * half) + epsilon)
    x = (x * scale * gain_ref[...]).astype(BF16)
    y = (y * scale * gain2_ref[...]).astype(BF16)

    shape = (EXPERTS * SLOTS, rows)
    slot = iota2(shape, 0)
    expert = divided(slot, 3)
    slot = slot - SLOTS * expert + first_slot(odd, core)
    first = (routes_ref[0:1, :] == expert).astype(F32)
    second = (routes_ref[1:2, :] == expert).astype(F32)
    member = first + second
    earlier = iota2((rows, rows), 0) < iota2((rows, rows), 1)
    place = dot(member.astype(BF16), one_hot(earlier))
    select = jnp.where(place == slot.astype(F32), member, 0.0)
    weight = first * weights_ref[0:1, :].astype(F32) + second * weights_ref[1:2, :].astype(F32)
    weight = jnp.sum(select * weight, axis=1, keepdims=True)
    weight = jnp.broadcast_to(weight, (EXPERTS * SLOTS, 128))
    select = select.astype(BF16)
    x, y = dot(select, x), dot(select, y)
    for k in range(EXPERTS):
        part = slice(k * SLOTS, (k + 1) * SLOTS)
        slot_ref[k, :, pl.ds(here, half)] = x[part].astype(BF16)
        slot_ref[k, :, pl.ds(there, half)] = y[part].astype(BF16)
        slot_ref[k, :, 2 * half :] = weight[part].astype(BF16)


def to_slots(place, own, other, mix, mix2, gain, gain2, routes, route_w):
    rows, half = own.shape
    vmem = pl.BlockSpec(memory_space=pltpu.VMEM)
    return pl.pallas_call(
        slots_kernel,
        name="slots",
        out_shape=(
            pltpu.VMEM((EXPERTS, SLOTS, 2 * half + 128), BF16),
            pltpu.VMEM((rows, half), BF16),
        ),
        in_specs=[pl.BlockSpec(memory_space=pltpu.SMEM)] * 2 + [vmem] * 8,
        out_specs=(vmem, vmem),
    )(
        place[0].reshape(1), place[1].reshape(1), in_vmem(own), in_vmem(other), in_vmem(mix), in_vmem(mix2),
        in_vmem(gain.reshape(1, half)), in_vmem(gain2.reshape(1, half)), in_vmem(routes.T),
        in_vmem(route_w.T),
    )


def home_kernel(z_ref, home_ref, after_ref, routes_ref, out_ref, rows_ref):
    odd = z_ref[0] & 1
    rows = after_ref.shape[0]
    count = home_ref.shape[0]
    for k in range(count):
        rows_ref[k * SLOTS : (k + 1) * SLOTS, :] = home_ref[k].astype(F32)
    shape = (rows, count * SLOTS)
    slot = iota2(shape, 1)
    source = divided(slot, 3)
    expert = source >> 1
    slot = slot - SLOTS * source + first_slot(odd, source & 1)
    member = (routes_ref[:, 0:1] == expert).astype(F32) + (routes_ref[:, 1:2] == expert).astype(F32)
    earlier = iota2((rows, rows), 1) < iota2((rows, rows), 0)
    place = dot(one_hot(earlier), member.astype(BF16))
    select = jnp.where(place == slot.astype(F32), member, 0.0).astype(BF16)
    total = after_ref[...].astype(F32) + dot(select, rows_ref[...].astype(BF16))
    out_ref[...] = total.astype(BF16)


def at_home(place, home, after, routes):
    vmem = pl.BlockSpec(memory_space=pltpu.VMEM)
    return pl.pallas_call(
        home_kernel,
        name="home",
        out_shape=jax.ShapeDtypeStruct(after.shape, BF16),
        in_specs=[pl.BlockSpec(memory_space=pltpu.SMEM)] + [vmem] * 3,
        out_specs=vmem,
        scratch_shapes=[pltpu.VMEM((home.shape[0] * SLOTS, home.shape[2]), F32)],
    )(place[1].reshape(1), in_vmem(home), in_vmem(after), in_vmem(routes))


def layer(
    tokens, state, norm_mix, w_query, w_key, w_value, w_out, norm_ffn, gate_vector,
    dense_gate, dense_up, dense_down, exp_gate, exp_up, exp_down, routes, route_w,
):
    core = lax.axis_index("tp")
    half = tokens.shape[1]
    hidden = dense_gate.shape[1]

    def fill(size):
        return jnp.zeros((size, half), BF16)

    other_x = swap(tokens)
    other_gain = swap(norm_ffn)
    packed = jnp.concatenate(
        [
            dense_gate.T,
            gate_vector[None],
            fill(PAD - hidden - 1),
            dense_up.T,
            fill(PAD - hidden),
            dense_down,
            fill(PAD - hidden),
        ],
        axis=0,
    )
    mine = (exp_gate[0].T, exp_up[0].T, exp_down[0])
    theirs = tuple(swap(weights) for weights in mine)

    mix, new_state = mixer(core, tokens, other_x, norm_mix, w_query, w_key, w_value, w_out, state)
    mix2 = swap(mix)
    place = (core, lax.axis_index("ep_0"))
    slot_rows, after = to_slots(
        place, tokens, other_x, mix, mix2, norm_ffn, other_gain, routes, route_w
    )
    at_plane = lax.all_to_all(slot_rows, "ep_0", 0, 0, tiled=True)
    pieces = [packed]
    for shift in (3, -3, -2, 2, 1, -1):
        pieces.append(along_z(packed, shift))
    pieces.append(along_z(pieces[2], -1))
    pieces2 = [swap(piece) for piece in pieces]
    chips = lax.axis_size(PLANE)
    copies = spread(core, at_plane, chips)
    gathered = lax.all_to_all(copies, PLANE, 0, 0, tiled=True)
    partial = experts_and_dense(
        core, gathered.reshape(chips * ROWS, MAIN), mine, theirs, pieces, pieces2, hidden
    )
    back = lax.all_to_all(partial.reshape(chips, ROWS, MAIN), PLANE, 0, 0, tiled=True)
    send = collect(core, back)
    home = lax.all_to_all(send, ("ep_0", "tp"), 0, 0, tiled=True)
    return (at_home(place, home, after, routes), new_state)


def solution(mesh):
    finer = Mesh(mesh.devices.reshape(8, 4, 4, mesh.shape["tp"]), ("ep_0", "ep_1", "ep_2", "tp"))
    in_specs = (
        P(EP, "tp"),
        P(EP, "tp", None, None),
        P(),
        P(None, "tp"),
        P(None, "tp"),
        P(None, "tp"),
        P("tp", None),
        P("tp"),
        P("tp"),
        P("tp", EP),
        P("tp", EP),
        P(EP, "tp"),
        P(EP, None, "tp"),
        P(EP, None, "tp"),
        P(EP, "tp", None),
        P(EP, None),
        P(EP, None),
    )
    out_specs = (P(EP, "tp"), P(EP, "tp", None, None))
    return jax.shard_map(layer, mesh=finer, in_specs=in_specs, out_specs=out_specs, check_vma=False)
```
